256 devices in a mesh: grp: 2 (over y), sp: 16 (over z), tp: 8 (over x, core).
Axes of the slice: x: 4, y: 2, z: 16, core: 2. Of those that a mesh axis runs over, the one named last changes fastest.
The devices are a block of a 4x16x16 slice.
Arguments:
- queries: bfloat16 [32768, 1024], P(('grp', 'sp'), 'tp'), parts along dimension 0, may hold values from -6 to 6
- keys: bfloat16 [32768, 256], P(('grp', 'sp')), parts along dimension 0, may hold values from -6 to 6
- values: bfloat16 [32768, 256], P(('grp', 'sp')), parts along dimension 0, may hold values from -6 to 6
- query_gain: float32 [128], replicated, may hold values from 1.2 to 6, as said below
- key_gain: float32 [128], replicated, may hold values from 1.2 to 6, as said below
- out_weight: bfloat16 [1024, 2048], replicated, may hold values from -6 to 6
- residual_in: bfloat16 [32768, 2048], P(('grp', 'sp', 'tp')), parts along dimension 0, may hold values from -6 to 6
- norm_gain: float32 [2048], replicated, may hold values from 0.1 to 1.9
- gate_weight: bfloat16 [2048, 2816], P('sp', 'tp'), may hold values from -0.125 to 0.125
- up_weight: bfloat16 [2048, 2816], P('sp', 'tp'), may hold values from -0.125 to 0.125
- down_weight: bfloat16 [2816, 2048], P('tp', 'sp'), may hold values from -0.109375 to 0.109375
Outputs:
- layer_out: bfloat16 [32768, 2048], P(('grp', 'sp', 'tp')), parts along dimension 0
The draws below stay inside these ranges and needn't reach their ends.
There are 2 independent parts, one for each index of `grp`. The reference program is written for one: setup_inputs(seed, part) draws one part's arguments, and reference() takes and returns one part's arrays. A program takes and returns all parts, laid end to end along the dimension named above; an argument that names none is the same for every part. Nothing has to cross between parts.
Inputs may be any that keep to these rules, and one draw needn't show every extreme that they name: `query_gain`: positive gains. `key_gain`: positive gains.
All inputs are finite; a program needn't handle non-finite values.
Results may differ from the reference program's by a relative error of at most 0.015.
The reference program's roundings to bfloat16 on the way (of `query_rot`, `key_rot`, `probs`, `attended`, `normed` and `hidden`) count: a program that leaves them out, or rounds other values in their place, can miss the bound.
Values may be sent and summed in bfloat16 or wider, within the bound.
A program may use at most 128 MiB of HBM per device.

```python
import jax
import jax.numpy as jnp
from jax import lax

D = 2048
HQ = 8
KV = 2
HD = 128
FF = 2816
GRID_W = 64
TOK_DEV = 1024
TOKENS = 16384


def shared_draw(key):
    key_rows = jax.random.truncated_normal(jax.random.fold_in(key, 1), -6.0, 6.0, (TOKENS, KV * HD), jnp.float32)
    query_rows = jax.random.truncated_normal(jax.random.fold_in(key, 2), -6.0, 6.0, (TOKENS, HQ * HD), jnp.float32)
    return (query_rows, key_rows)


def draw_queries(key, part):
    return shared_draw(key)[0].astype(jnp.bfloat16)


def draw_keys(key, part):
    return shared_draw(key)[1].astype(jnp.bfloat16)


def draw_query_gain(key, part):
    return jax.random.uniform(jax.random.fold_in(key, 11), (HD,), jnp.float32, 1.2, 1.7)


def draw_key_gain(key, part):
    return jax.random.uniform(jax.random.fold_in(key, 12), (HD,), jnp.float32, 1.2, 1.7)


def block_levels(own_key, extent, pieces, low, largest):
    level = 1.0
    for dim, parts in pieces:
        draws = jax.random.uniform(jax.random.fold_in(jax.random.fold_in(own_key, 6), dim), (parts,), jnp.float32, low / len(pieces), largest / len(pieces))
        level = level * jnp.repeat(jnp.exp(draws), extent[dim] // parts).reshape((-1,) + (1,) * (len(extent) - 1 - dim))
    return level


def centred(own_key, extent, deviation, bound, shards=(), kind=jnp.bfloat16):
    result = jax.random.normal(own_key, extent, jnp.float32) * deviation
    if len(shards) > 0:
        result = block_levels(own_key, extent, shards, -0.22, 0.18) * result
    return jnp.clip(result, min=-bound, max=bound).astype(kind)


def setup_inputs(seed: int = 0, part: int = 0) -> dict:
    arg_keys = jax.random.split(jax.random.key(seed), 12)
    part_keys = jax.random.split(jax.random.fold_in(arg_keys[11], part), 12)
    queries = draw_queries(jax.random.fold_in(jax.random.fold_in(arg_keys[11], part), 71), part)
    keys = draw_keys(jax.random.fold_in(jax.random.fold_in(arg_keys[11], part), 71), part)
    values = centred(part_keys[2], (TOKENS, KV * HD), 1.0, 6.0, ((0, 16),))
    query_gain = draw_query_gain(jax.random.fold_in(arg_keys[11], 71), part)
    key_gain = draw_key_gain(jax.random.fold_in(arg_keys[11], 71), part)
    out_weight = centred(arg_keys[5], (HQ * HD, D), 0.4, 6.0)
    residual_in = centred(part_keys[6], (TOKENS, D), 1.0, 6.0, ((0, 128),))
    norm_gain = jnp.clip(1.0 + 0.18 * jax.random.normal(arg_keys[7], (D,), jnp.float32), 0.1, 1.9)
    gate_weight = centred(arg_keys[8], (D, FF), D ** -0.5, 0.125, ((0, 16), (1, 8)))
    up_weight = centred(arg_keys[9], (D, FF), D ** -0.5, 0.125, ((0, 16), (1, 8)))
    down_weight = centred(arg_keys[10], (FF, D), FF ** -0.5, 0.109375, ((0, 8), (1, 16)))
    return {"queries": queries, "keys": keys, "values": values, "query_gain": query_gain, "key_gain": key_gain, "out_weight": out_weight, "residual_in": residual_in, "norm_gain": norm_gain, "gate_weight": gate_weight, "up_weight": up_weight, "down_weight": down_weight}


def rotate(widened, positions):
    half = HD // 2
    inverse = 10000.0 ** (-jnp.arange(0, half, 2, dtype=jnp.float32) / half)
    grid_row = (positions // GRID_W).astype(jnp.float32)
    grid_col = (positions % GRID_W).astype(jnp.float32)
    angles = jnp.concatenate([grid_row[:, None] * inverse[None], grid_col[:, None] * inverse[None]], axis=-1)
    cosine = jnp.cos(angles)[:, None, :]
    sine = jnp.sin(angles)[:, None, :]
    pairs = widened.reshape(widened.shape[0], widened.shape[1], half, 2)
    first = pairs[..., 0]
    second = pairs[..., 1]
    turned = jnp.stack([first * cosine - second * sine, first * sine + second * cosine], axis=-1)
    return turned.reshape(widened.shape)

def prepare(source, gain, positions, heads):
    widened = source.astype(jnp.float32).reshape(source.shape[0], heads, HD)
    widened = widened * lax.rsqrt(lax.optimization_barrier(jnp.mean(widened * widened, axis=-1, keepdims=True)) + 1e-06) * gain
    return rotate(widened, positions).astype(jnp.bfloat16)

def reference(queries, keys, values, query_gain, key_gain, out_weight, residual_in, norm_gain, gate_weight, up_weight, down_weight):
    positions = jnp.arange(TOKENS, dtype=jnp.int32)
    query_rot = prepare(queries, query_gain, positions, HQ).transpose(1, 0, 2)
    key_rot = prepare(keys, key_gain, positions, KV).transpose(1, 0, 2)
    value_heads = values.reshape(TOKENS, KV, HD).transpose(1, 0, 2)
    group = HQ // KV
    scale = HD ** (-0.5)

    def one_head(head):
        key_block = key_rot[head // group]
        value_block = value_heads[head // group]
        query_blocks = query_rot[head].reshape(TOKENS // TOK_DEV, TOK_DEV, HD)

        def one_block(query_block):
            scores = jnp.dot(query_block, key_block.T, preferred_element_type=jnp.float32) * scale
            peak = lax.optimization_barrier(jnp.max(scores, axis=1, keepdims=True))
            raised = jnp.exp(scores - peak)
            denominator = lax.optimization_barrier(jnp.sum(raised, axis=1, keepdims=True))
            probs = raised.astype(jnp.bfloat16)
            mixed = jnp.dot(probs, value_block, preferred_element_type=jnp.float32)
            return (mixed / denominator).astype(jnp.bfloat16)
        return lax.map(one_block, query_blocks).reshape(TOKENS, HD)
    attended = lax.map(one_head, jnp.arange(HQ, dtype=jnp.int32))
    attended = attended.transpose(1, 0, 2).reshape(TOKENS, HQ * HD)
    middle = residual_in.astype(jnp.float32) + jnp.dot(attended, out_weight, preferred_element_type=jnp.float32)
    normed = middle * lax.rsqrt(lax.optimization_barrier(jnp.mean(middle * middle, axis=-1, keepdims=True)) + 1e-06) * norm_gain
    normed = normed.astype(jnp.bfloat16)
    gate_act = jnp.dot(normed, gate_weight, preferred_element_type=jnp.float32)
    up_act = jnp.dot(normed, up_weight, preferred_element_type=jnp.float32)
    hidden = (jax.nn.silu(gate_act) * up_act).astype(jnp.bfloat16)
    mixer_out = jnp.dot(hidden, down_weight, preferred_element_type=jnp.float32)
    return (middle + mixer_out).astype(jnp.bfloat16)
```

```python
import functools
import math

import jax
import jax.numpy as jnp
from jax import lax
from jax.experimental import pallas as pl
from jax.experimental.pallas import tpu as pltpu
from jax.sharding import PartitionSpec as P

HQ = 8
KV = 2
HD = 128
GRID_W = 64
MESH = pl.DeviceIdType.MESH
F32 = jnp.float32
BF16 = jnp.bfloat16
ROWS_ATT = 256
ROWS_FF = 256


def layer_kernel(
    n,
    n_tp,
    q_ref,
    k_ref,
    v_ref,
    qg_ref,
    kg_ref,
    inv_ref,
    ow_hbm,
    res_ref,
    ng_ref,
    gate_ref,
    up_ref,
    down_ref,
    out_ref,
    kv,
    qrot,
    acc,
    mx,
    ls,
    cosr,
    sinr,
    gw,
    uw,
    dw,
    ow,
    res,
    att,
    nrm,
    mid,
    hid,
    part,
    d2s,
    d2r,
    s1s,
    s1r,
    s2s,
    s2r,
    yk,
    zk,
    ow_sem,
    kv_ss,
    kv_rs,
    kd_ss,
    kd_rs,
    w_ss,
    w_rs,
    a_ss,
    a_rs,
    r_ss,
    r_rs,
    t_ss,
    t_rs,
):
    me = lax.axis_index("sp")
    tp = lax.axis_index("tp")
    core = lax.rem(tp, 2)
    x = tp // 2
    tok = q_ref.shape[0]
    d = res_ref.shape[1]
    own_rows = res_ref.shape[0]
    half_n = n // 2
    kv_head = tp // (n_tp // KV)

    def wrap(i):
        return lax.rem(i + n, n)

    right = wrap(me + 1)
    left = wrap(me - 1)
    n1x = x + 1 - 2 * lax.rem(x, 2)
    n2x = 3 - x
    dgx = 3 - n1x
    mate = x * 2 + 1 - core
    n1 = n1x * 2 + core
    n2 = n2x * 2 + core
    dg = dgx * 2 + core
    to_right, to_left = {"sp": right}, {"sp": left}
    to_mate, to_n1, to_n2 = {"tp": mate}, {"tp": n1}, {"tp": n2}

    def remote(src, dst, ss, rs, dev):
        return pltpu.make_async_remote_copy(
            src_ref=src, dst_ref=dst, send_sem=ss, recv_sem=rs, device_id=dev, device_id_type=MESH
        )

    load_ow = pltpu.make_async_copy(ow_hbm, ow, ow_sem)
    load_ow.start()

    barrier = pltpu.get_barrier_semaphore()
    for dev in (to_right, to_left, to_mate, to_n1, to_n2):
        pl.semaphore_signal(barrier, inc=1, device_id=dev, device_id_type=MESH)

    grid_rows = tok // GRID_W
    lane = lax.broadcasted_iota(jnp.int32, (GRID_W, HD), 1)
    row_pos = (me * grid_rows + lax.broadcasted_iota(jnp.int32, (grid_rows, HD), 0)).astype(F32)
    row_ang = row_pos * inv_ref[...]
    cosr[...] = jnp.cos(row_ang)
    sinr[...] = jnp.sin(row_ang)
    col_ang = lax.broadcasted_iota(jnp.int32, (GRID_W, HD), 0).astype(F32) * inv_ref[...]
    cos_col = jnp.cos(col_ang)
    sin_col = jnp.sin(col_ang)
    even = lax.rem(lane, 2) == 0
    by_row = lane < HD // 2

    def turned(source, gain, i):
        v = source.astype(F32)
        v = v * lax.rsqrt(jnp.mean(v * v, axis=-1, keepdims=True) + 1e-06) * gain
        cosine = jnp.where(by_row, cosr[pl.ds(i, 1), :], cos_col)
        sine = jnp.where(by_row, sinr[pl.ds(i, 1), :], sin_col)
        swapped = jnp.where(even, pltpu.roll(v, HD - 1, 1), pltpu.roll(v, 1, 1))
        signed = jnp.where(even, -sine, sine)
        return (v * cosine + swapped * signed).astype(BF16)

    kv_lanes = pl.ds(pl.multiple_of(kv_head * HD, HD), HD)

    def prep_k(i, _):
        rows = pl.ds(pl.multiple_of(i * GRID_W, GRID_W), GRID_W)
        kv[me, rows, 0:HD] = turned(k_ref[rows, kv_lanes], kg_ref[...], i)
        kv[me, rows, HD : 2 * HD] = v_ref[rows, kv_lanes]
        return 0

    lax.fori_loop(0, grid_rows, prep_k, 0)
    pl.semaphore_wait(barrier, 5)

    quarter = tok // 4
    slab = tok // 2

    def q_slot(b, a, c):
        return kv.at[b, pl.ds(pl.multiple_of((2 * a + c) * quarter, quarter), quarter), :]

    def kv_ring(direction, t, a):
        b = wrap(me - t) if direction == 0 else wrap(me + t)
        s = q_slot(b, a, core)
        return remote(
            s, s, kv_ss.at[direction, t, a], kv_rs.at[direction, t, a], (to_right, to_left)[direction]
        )

    def kv_send(direction, t, a):
        b = wrap(me - t) if direction == 0 else wrap(me + t)
        s = q_slot(b, a, core)
        return remote(
            s,
            s,
            kv_ss.at[direction, t, a],
            kv_rs.at[direction, t + 1, a],
            (to_right, to_left)[direction],
        )

    def kv_mate(direction, t, a, whose):
        b = wrap(me - t) if direction == 0 else wrap(me + t)
        s = q_slot(b, a, whose)
        return remote(s, s, kd_ss.at[direction, t, a], kd_rs.at[direction, t, a], to_mate)

    for a in range(2):
        for direction in range(2):
            kv_send(direction, 0, a).start()

    half_d = d // 2

    def res_slot(j, h=None):
        rows = pl.ds(pl.multiple_of(j * own_rows, own_rows), own_rows)
        if h is None:
            return res.at[rows, :]
        return res.at[rows, h * half_d : (h + 1) * half_d]

    def att_slot(j, h=None):
        lanes = pl.ds(pl.multiple_of(j * HD, HD), HD)
        if h is None:
            return att.at[:, lanes]
        return att.at[h * slab : (h + 1) * slab, lanes]

    def gather_steps(slot, ss, rs):
        def pair(s, i, dev):
            return remote(s, s, ss.at[i], rs.at[i], dev)

        def own(side, h):
            return pair(slot(tp, h), side * 2 + h, (to_n1, to_n2)[side])

        def arrived(side, h):
            return pair(slot((n1, n2)[side], h), side * 2 + h, (to_n1, to_n2)[side])

        def onward(h):
            return pair(slot((n1, n2)[h], h), 4 + h, (to_n2, to_n1)[h])

        def diag_arrived(h):
            return pair(slot(dg, h), 4 + h, (to_n2, to_n1)[h])

        def mates(i, j):
            return pair(slot(j), 6 + i, to_mate)

        def mate_arrived(i, j):
            return pair(slot(j + 1 - 2 * core), 6 + i, to_mate)

        def first():
            for h in (0, 1):
                own(0, h).start()
                own(1, 1 - h).start()
            mates(0, tp).start()

        def second():
            for side, h in ((0, 0), (1, 1), (0, 1), (1, 0)):
                arrived(side, h).wait_recv()
                if side == h:
                    onward(h).start()
            mates(1, n1).start()
            mates(2, n2).start()

        def third():
            diag_arrived(0).wait_recv()
            diag_arrived(1).wait_recv()
            mates(3, dg).start()

        def fourth():
            for i, j in enumerate((tp, n1, n2, dg)):
                mate_arrived(i, j).wait_recv()

        def sent():
            for side in (0, 1):
                for h in (0, 1):
                    own(side, h).wait_send()
            for h in (0, 1):
                onward(h).wait_send()
            for i, j in enumerate((tp, n1, n2, dg)):
                mates(i, j).wait_send()

        return first, second, third, fourth, sent

    res_first, res_second, res_third, res_fourth, res_sent = gather_steps(res_slot, r_ss, r_rs)
    att_first, att_second, att_third, att_fourth, att_sent = gather_steps(att_slot, a_ss, a_rs)

    gk = gate_ref.shape[0]
    ff = down_ref.shape[0]

    def w_slot(which, b):
        if which == 2:
            return dw.at[pl.ds(pl.multiple_of(b * ff, ff), ff), :]
        return (gw, uw)[which].at[pl.ds(pl.multiple_of(b * gk, gk), gk), :]

    def w_copy(which, direction, t, late):
        b = wrap(me - t) if direction == 0 else wrap(me + t)
        s = w_slot(which, b)
        return remote(
            s,
            s,
            w_ss.at[which, direction, t],
            w_rs.at[which, direction, t + late],
            (to_right, to_left)[direction],
        )

    def w_start(whiches):
        for which in whiches:
            for direction in range(2):
                w_copy(which, direction, 0, 1).start()

    def w_step(whiches, t):
        for direction in range(2):
            for which in whiches:
                w_copy(which, direction, t, 0).wait_recv()

                @pl.when((t < half_n - 1) | (core == direction))
                def _():
                    w_copy(which, direction, t, 1).start()

    def w_last(whiches):
        for direction in range(2):

            @pl.when(core == direction)
            def _():
                for which in whiches:
                    w_copy(which, direction, half_n, 0).wait_recv()

    def w_sent(whiches):
        def one(t, _):
            for direction in range(2):
                for which in whiches:

                    @pl.when((t < half_n - 1) | (core == direction))
                    def _():
                        w_copy(which, direction, t, 1).wait_send()

            return 0

        lax.fori_loop(0, half_n, one, 0)

    def prep_q(i, _):
        rows = pl.ds(pl.multiple_of(i * GRID_W, GRID_W), GRID_W)
        qrot[rows, :] = turned(q_ref[rows, :], qg_ref[...], i)
        return 0

    lax.fori_loop(0, grid_rows, prep_q, 0)
    res_slot(tp)[...] = res_ref[...]
    w_slot(0, me)[...] = gate_ref[...]
    w_slot(1, me)[...] = up_ref[...]
    w_slot(2, me)[...] = down_ref[...]
    mx[...] = jnp.full(mx.shape, -1e30, F32)
    ls[...] = jnp.zeros(ls.shape, F32)
    acc[...] = jnp.zeros(acc.shape, F32)

    factor = HD ** (-0.5) * math.log2(math.e)

    def attend(b1, h1, b2, h2):
        def one(i, _):
            rows = pl.ds(pl.multiple_of(i * ROWS_ATT, ROWS_ATT), ROWS_ATT)
            q = qrot[rows, :]
            r1 = pl.ds(pl.multiple_of(h1 * slab, slab), slab)
            r2 = pl.ds(pl.multiple_of(h2 * slab, slab), slab)
            dims = (((1,), (1,)), ((), ()))
            scores = [
                lax.dot_general(q, kv[b, r, 0:HD], dims, preferred_element_type=F32)
                for b, r in ((b1, r1), (b2, r2))
            ]
            top = None
            for s in scores:
                for j in range(slab // HD):
                    tile = s[:, j * HD : (j + 1) * HD]
                    top = tile if top is None else jnp.maximum(top, tile)
            old = mx[rows, :]
            new = jnp.maximum(old, jnp.max(top, axis=1, keepdims=True))
            mx[rows, :] = new
            alpha = jnp.exp2((old - new) * factor)
            base = new[:, 0:1]
            total = ls[rows, :] * alpha
            weighted = acc[rows, :] * alpha
            for s, (b, r) in zip(scores, ((b1, r1), (b2, r2))):
                raised = jnp.exp2((s - base) * factor)
                for j in range(slab // HD):
                    total = total + raised[:, j * HD : (j + 1) * HD]
                weighted = weighted + jnp.dot(
                    raised.astype(BF16), kv[b, r, HD : 2 * HD], preferred_element_type=F32
                )
            ls[rows, :] = total
            acc[rows, :] = weighted
            return 0

        lax.fori_loop(0, tok // ROWS_ATT, one, 0)

    def kv_take(t, a):
        for direction in range(2):
            kv_ring(direction, t, a).wait_recv()

            @pl.when((t < half_n - 1) | (core == direction))
            def _():
                kv_send(direction, t, a).start()

            kv_mate(direction, t, a, core).start()

    def mate_take(t, a):
        for direction in range(2):
            kv_mate(direction, t, a, 1 - core).wait_recv()

    kv_take(1, 0)
    res_first()
    attend(me, 0, me, 1)

    def phase(p, _):
        t, a = (p + 1) // 2, lax.rem(p + 1, 2)
        tb, ab = p // 2, lax.rem(p, 2)
        kv_take(t, a)

        @pl.when(p == 6)
        def _():
            res_second()

        @pl.when(p == 10)
        def _():
            res_third()

        @pl.when(p == 2 * half_n - 2)
        def _():
            w_start((0, 1))

        mate_take(tb, ab)
        attend(wrap(me - tb), ab, wrap(me + tb), ab)
        return 0

    lax.fori_loop(2, 2 * half_n - 1, phase, 0)
    for direction in range(2):

        @pl.when(core == direction)
        def _():
            for a in range(2):
                kv_ring(direction, half_n, a).wait_recv()
                kv_mate(direction, half_n, a, core).start()

    mate_take(half_n - 1, 1)
    attend(wrap(me - half_n + 1), 1, wrap(me + half_n - 1), 1)
    w_step((0, 1), 1)
    for direction in range(2):

        @pl.when(core == 1 - direction)
        def _():
            for a in range(2):
                kv_mate(direction, half_n, a, 1 - core).wait_recv()

    attend(wrap(me + half_n), 0, wrap(me + half_n), 1)

    def finish(i, _):
        rows = pl.ds(pl.multiple_of(i * ROWS_ATT, ROWS_ATT), ROWS_ATT)
        below = jnp.sum(ls[rows, :], axis=1, keepdims=True)
        att[rows, pl.ds(pl.multiple_of(tp * HD, HD), HD)] = (acc[rows, :] / below).astype(BF16)
        return 0

    lax.fori_loop(0, tok // ROWS_ATT, finish, 0)
    w_step((0, 1), 2)
    att_first()
    res_fourth()
    load_ow.wait()
    att_second()
    w_step((0, 1), 3)
    att_third()
    att_fourth()

    def project(i, _):
        rows = pl.ds(pl.multiple_of(i * ROWS_FF, ROWS_FF), ROWS_FF)
        middle = res[rows, :].astype(F32) + jnp.dot(
            att[rows, :], ow[...], preferred_element_type=F32
        )
        scale = lax.rsqrt(jnp.mean(middle * middle, axis=-1, keepdims=True) + 1e-06)
        nrm[rows, :] = (middle * scale * ng_ref[...]).astype(BF16)
        held = ROWS_FF // own_rows
        for j in range(held):

            @pl.when(tp == i * held + j)
            def _():
                mid[...] = middle[j * own_rows : (j + 1) * own_rows, :]

        @pl.when(i + 4 < half_n)
        def _():
            w_step((0, 1), i + 4)

        return 0

    lax.fori_loop(0, tok // ROWS_FF, project, 0)
    w_start((2,))
    w_last((0, 1))

    def units(i, _):
        rows = pl.ds(pl.multiple_of(i * ROWS_FF, ROWS_FF), ROWS_FF)
        n_rows = nrm[rows, :]
        gate = jnp.dot(n_rows, gw[...], preferred_element_type=F32)
        up = jnp.dot(n_rows, uw[...], preferred_element_type=F32)
        hid[rows, :] = (gate / (1.0 + jnp.exp(-gate)) * up).astype(BF16)

        @pl.when(i == 1)
        def _():
            w_step((2,), 1)

        @pl.when(i == 3)
        def _():
            w_step((2,), 2)

        return 0

    lax.fori_loop(0, tok // ROWS_FF, units, 0)

    near = (n1x, n2x)
    far = (n2x, n1x)
    to_near = (to_n1, to_n2)
    to_far = (to_n2, to_n1)

    def col_block(g, k):
        return wrap(me - k) if g == 0 else wrap(me + k + 1)

    def d2_copy(g, k):
        return remote(d2s.at[g, k], d2r.at[g, k], t_ss.at[0, g, k], t_rs.at[0, g, k], to_mate)

    def s1_copy(g, k):
        return remote(s1s.at[g, k], s1r.at[g, k], t_ss.at[1, g, k], t_rs.at[1, g, k], to_near[g])

    def s2_copy(g, k):
        return remote(s2s.at[g, k], s2r.at[g, k], t_ss.at[2, g, k], t_rs.at[2, g, k], to_far[g])

    def stage0(k):
        for g in range(2):
            b = col_block(g, k)
            part[g, lax.rem(k, 2)] = jnp.dot(
                hid[...],
                dw[pl.ds(pl.multiple_of(b * ff, ff), ff), :],
                preferred_element_type=F32,
            )
            for c in range(4):
                at = pl.ds(pl.multiple_of((c * 2 + 1 - core) * own_rows, own_rows), own_rows)
                d2s[g, k, c * own_rows : (c + 1) * own_rows, :] = part[g, lax.rem(k, 2), at, :].astype(
                    BF16
                )
            d2_copy(g, k).start()

    def stage1(k):
        slot = lax.rem(k, 2)
        for g in range(2):
            d2_copy(g, k).wait_recv()

            def summed(c):
                mine = pl.ds(pl.multiple_of((c * 2 + core) * own_rows, own_rows), own_rows)
                theirs = pl.ds(pl.multiple_of(c * own_rows, own_rows), own_rows)
                return part[g, slot, mine, :] + d2r[g, k, theirs, :].astype(F32)

            s1s[g, k, 0:own_rows, :] = summed(near[g]).astype(BF16)
            s1s[g, k, own_rows : 2 * own_rows, :] = summed(dgx).astype(BF16)
            yk[g, slot, 0] = summed(x)
            yk[g, slot, 1] = summed(far[g])
            s1_copy(g, k).start()

    def stage2(k):
        slot = lax.rem(k, 2)
        for g in range(2):
            s1_copy(g, k).wait_recv()
            s2s[g, k] = (
                yk[g, slot, 1] + s1r[g, k, own_rows : 2 * own_rows, :].astype(F32)
            ).astype(BF16)
            zk[g, slot] = yk[g, slot, 0] + s1r[g, k, 0:own_rows, :].astype(F32)
            s2_copy(g, k).start()

    def stage3(k):
        slot = lax.rem(k, 2)
        for g in range(2):
            s2_copy(g, k).wait_recv()
            lanes = pl.ds(pl.multiple_of(col_block(g, k) * HD, HD), HD)
            out_ref[:, lanes] = (mid[:, lanes] + zk[g, slot] + s2r[g, k].astype(F32)).astype(BF16)

    def columns(k, _):
        @pl.when(k >= 3)
        def _():
            stage3(k - 3)

        @pl.when((k >= 2) & (k < half_n + 2))
        def _():
            stage2(k - 2)

        @pl.when((k >= 1) & (k < half_n + 1))
        def _():
            stage1(k - 1)

        @pl.when(k < half_n)
        def _():
            stage0(k)

        @pl.when(k + 3 < half_n)
        def _():
            w_step((2,), k + 3)

        @pl.when(k + 3 == half_n)
        def _():
            w_last((2,))

        return 0

    lax.fori_loop(0, half_n + 3, columns, 0)

    def kv_sent(t, _):
        for a in range(2):
            for direction in range(2):

                @pl.when((t < half_n - 1) | (core == direction))
                def _():
                    kv_send(direction, t, a).wait_send()

                @pl.when(t > 0)
                def _():
                    kv_mate(direction, t, a, core).wait_send()

        return 0

    lax.fori_loop(0, half_n, kv_sent, 0)
    for direction in range(2):

        @pl.when(core == direction)
        def _():
            for a in range(2):
                kv_mate(direction, half_n, a, core).wait_send()

    w_sent((0, 1, 2))
    res_sent()
    att_sent()

    def sums_sent(k, _):
        for g in range(2):
            d2_copy(g, k).wait_send()
            s1_copy(g, k).wait_send()
            s2_copy(g, k).wait_send()
        return 0

    lax.fori_loop(0, half_n, sums_sent, 0)


def local(
    n,
    n_tp,
    queries,
    keys,
    values,
    query_gain,
    key_gain,
    out_weight,
    residual_in,
    norm_gain,
    gate_weight,
    up_weight,
    down_weight,
):
    tok = queries.shape[0]
    own_rows, d = residual_in.shape
    ff = down_weight.shape[0]
    gk = gate_weight.shape[0]
    half = HD // 2
    half_n = n // 2
    inverse = 10000.0 ** (-jnp.arange(0, half, 2, dtype=F32) / half)
    inverse = jnp.tile(jnp.repeat(inverse, 2), 2)[None]
    vmem = pl.BlockSpec(memory_space=pltpu.VMEM)
    dma = pltpu.SemaphoreType.DMA
    scratch = [
        pltpu.VMEM((n, tok, 2 * HD), BF16),
        pltpu.VMEM((tok, HD), BF16),
        pltpu.VMEM((tok, HD), F32),
        pltpu.VMEM((tok, HD), F32),
        pltpu.VMEM((tok, HD), F32),
        pltpu.VMEM((tok // GRID_W, HD), F32),
        pltpu.VMEM((tok // GRID_W, HD), F32),
        pltpu.VMEM((n * gk, ff), BF16),
        pltpu.VMEM((n * gk, ff), BF16),
        pltpu.VMEM((n * ff, HD), BF16),
        pltpu.VMEM(out_weight.shape, BF16),
        pltpu.VMEM((tok, d), BF16),
        pltpu.VMEM((tok, HQ * HD), BF16),
        pltpu.VMEM((tok, d), BF16),
        pltpu.VMEM((own_rows, d), F32),
        pltpu.VMEM((tok, ff), BF16),
        pltpu.VMEM((2, 2, tok, HD), F32),
        pltpu.VMEM((2, half_n, tok // 2, HD), BF16),
        pltpu.VMEM((2, half_n, tok // 2, HD), BF16),
        pltpu.VMEM((2, half_n, 2 * own_rows, HD), BF16),
        pltpu.VMEM((2, half_n, 2 * own_rows, HD), BF16),
        pltpu.VMEM((2, half_n, own_rows, HD), BF16),
        pltpu.VMEM((2, half_n, own_rows, HD), BF16),
        pltpu.VMEM((2, 2, 2, own_rows, HD), F32),
        pltpu.VMEM((2, 2, own_rows, HD), F32),
        dma,
        dma((2, half_n + 1, 2)),
        dma((2, half_n + 1, 2)),
        dma((2, half_n + 1, 2)),
        dma((2, half_n + 1, 2)),
        dma((3, 2, half_n + 1)),
        dma((3, 2, half_n + 1)),
        dma((10,)),
        dma((10,)),
        dma((10,)),
        dma((10,)),
        dma((3, 2, half_n)),
        dma((3, 2, half_n)),
    ]
    specs = [vmem] * 12
    specs[6] = pl.BlockSpec(memory_space=pl.ANY)
    return pl.pallas_call(
        functools.partial(layer_kernel, n, n_tp),
        out_shape=jax.ShapeDtypeStruct((own_rows, d), BF16),
        in_specs=specs,
        out_specs=vmem,
        scratch_shapes=scratch,
        compiler_params=pltpu.CompilerParams(
            collective_id=0, has_side_effects=True, vmem_limit_bytes=67043328
        ),
        name="layer",
    )(
        queries,
        keys,
        values,
        query_gain[None],
        key_gain[None],
        inverse,
        out_weight,
        residual_in,
        norm_gain[None],
        gate_weight,
        up_weight,
        down_weight,
    )


def solution(mesh):
    placed = (
        P(("grp", "sp"), "tp"),
        P(("grp", "sp"), None),
        P(("grp", "sp"), None),
        P(),
        P(),
        P(),
        P(("grp", "sp", "tp"), None),
        P(),
        P("sp", "tp"),
        P("sp", "tp"),
        P("tp", "sp"),
    )
    return jax.shard_map(
        functools.partial(local, mesh.shape["sp"], mesh.shape["tp"]),
        mesh=mesh,
        in_specs=placed,
        out_specs=P(("grp", "sp", "tp"), None),
        check_vma=False,
    )
```

```python
import functools
import math

import jax
import jax.numpy as jnp
import numpy as np
from jax import lax
from jax.experimental import pallas as pl
from jax.experimental.pallas import tpu as pltpu
from jax.sharding import PartitionSpec as P

HQ = 8
KV = 2
HD = 128
GRID_W = 64
MESH = pl.DeviceIdType.MESH
F32 = jnp.float32
BF16 = jnp.bfloat16
ROWS_ATT = 256
ROWS_FF = 256
TILES = 4


def scoped(name):
    def wrapped(f):
        def call(*args):
            with jax.named_scope(name):
                return f(*args)

        return call

    return wrapped


def layer_kernel(
    n,
    n_tp,
    q_ref,
    k_ref,
    v_ref,
    qg_ref,
    kg_ref,
    inv_ref,
    ow_hbm,
    res_ref,
    ng_ref,
    gate_ref,
    up_ref,
    down_ref,
    out_ref,
    kv,
    qrot,
    acc,
    mx,
    ls,
    sa,
    sb,
    ta,
    tb,
    cosr,
    sinr,
    gu,
    dw,
    ow,
    res,
    att,
    nrm,
    mid,
    hid,
    part,
    kept,
    d2s,
    d2r,
    s1s,
    s1r,
    s2s,
    s2r,
    yk,
    zk,
    ow_sem,
    kv_ss,
    kv_rs,
    kx_ss,
    kx_rs,
    kd_ss,
    kd_rs,
    w_ss,
    w_rs,
    y_ss,
    y_rs,
    a_ss,
    a_rs,
    r_ss,
    r_rs,
    t_ss,
    t_rs,
):
    me = lax.axis_index("sp")
    tp = lax.axis_index("tp")
    grp = lax.axis_index("grp")
    odd = lax.rem(grp, 2)
    core = lax.rem(tp, 2)
    x = tp // 2
    tok = q_ref.shape[0]
    d = res_ref.shape[1]
    own_rows = res_ref.shape[0]
    half_n = n // 2
    kv_head = tp // (n_tp // KV)

    def wrap(i):
        return lax.rem(i + n, n)

    right = wrap(me + 1)
    left = wrap(me - 1)
    n1x = x + 1 - 2 * lax.rem(x, 2)
    n2x = 3 - x
    dgx = 3 - n1x
    mate = x * 2 + 1 - core
    n1 = n1x * 2 + core
    n2 = n2x * 2 + core
    dg = dgx * 2 + core
    to_right, to_left = {"sp": right}, {"sp": left}
    to_mate, to_n1, to_n2 = {"tp": mate}, {"tp": n1}, {"tp": n2}
    to_twin = {"grp": grp + 1 - 2 * odd}

    def remote(src, dst, ss, rs, dev):
        return pltpu.make_async_remote_copy(
            src_ref=src, dst_ref=dst, send_sem=ss, recv_sem=rs, device_id=dev, device_id_type=MESH
        )

    load_ow = pltpu.make_async_copy(ow_hbm, ow, ow_sem)
    load_ow.start()

    barrier = pltpu.get_barrier_semaphore()
    for dev in (to_right, to_left, to_mate, to_n1, to_n2, to_twin):
        pl.semaphore_signal(barrier, inc=1, device_id=dev, device_id_type=MESH)

    grid_rows = tok // GRID_W
    lane = lax.broadcasted_iota(jnp.int32, (GRID_W, HD), 1)
    row_pos = (me * grid_rows + lax.broadcasted_iota(jnp.int32, (grid_rows, HD), 0)).astype(F32)
    row_ang = row_pos * inv_ref[...]
    cosr[...] = jnp.cos(row_ang)
    sinr[...] = jnp.sin(row_ang)
    col_ang = lax.broadcasted_iota(jnp.int32, (GRID_W, HD), 0).astype(F32) * inv_ref[...]
    cos_col = jnp.cos(col_ang)
    sin_col = jnp.sin(col_ang)
    even = lax.rem(lane, 2) == 0
    by_row = lane < HD // 2

    def turned(source, gain, i):
        v = source.astype(F32)
        v = v * lax.rsqrt(jnp.mean(v * v, axis=-1, keepdims=True) + 1e-06) * gain
        cosine = jnp.where(by_row, cosr[pl.ds(i, 1), :], cos_col)
        sine = jnp.where(by_row, sinr[pl.ds(i, 1), :], sin_col)
        swapped = jnp.where(even, pltpu.roll(v, HD - 1, 1), pltpu.roll(v, 1, 1))
        signed = jnp.where(even, -sine, sine)
        return (v * cosine + swapped * signed).astype(BF16)

    kv_lanes = pl.ds(pl.multiple_of(kv_head * HD, HD), HD)

    def prep_k(o, _):
        for u in range(TILES):
            i = o * TILES + u
            rows = pl.ds(pl.multiple_of(i * GRID_W, GRID_W), GRID_W)
            kv[me, rows, 0:HD] = turned(k_ref[rows, kv_lanes], kg_ref[...], i)
            kv[me, rows, HD : 2 * HD] = v_ref[rows, kv_lanes]
        return 0

    with jax.named_scope("prepk"):
        lax.fori_loop(0, grid_rows // TILES, prep_k, 0)
        res[pl.ds(pl.multiple_of(tp * own_rows, own_rows), own_rows), :] = res_ref[...]
    with jax.named_scope("barrier"):
        pl.semaphore_wait(barrier, 6)

    quarter = tok // 4
    slab = tok // 2

    side = lax.rem(x, 2)
    share = quarter * 5 // 16
    sizes = (share, share, quarter - 2 * share)

    def block_at(direction, t):
        return wrap(me - t) if direction == 0 else wrap(me + t)

    def piece(direction, t, a, c, which):
        start = (side * share, (1 - side) * share, 2 * share)[which]
        at = pl.multiple_of((2 * a + c) * quarter + start, 16)
        return kv.at[block_at(direction, t), pl.ds(at, sizes[which]), :]

    def kv_ring(direction, t, a, which, late):
        s = piece(direction, t, a, core, which)
        return remote(
            s,
            s,
            kv_ss.at[direction, t, a, which // 2],
            kv_rs.at[direction, t + late, a, which // 2],
            (to_right, to_left)[direction],
        )

    def kv_near(direction, t, a, which):
        s = piece(direction, t, a, core, which)
        return remote(s, s, kx_ss.at[direction, t, a], kx_rs.at[direction, t, a], to_n1)

    def kv_mate(direction, t, a, c, which):
        s = piece(direction, t, a, c, which)
        return remote(
            s, s, kd_ss.at[direction, t, a, which], kd_rs.at[direction, t, a, which], to_mate
        )

    for a in range(2):
        for which in (0, 2):
            for direction in range(2):
                kv_ring(direction, 0, a, which, 1).start()

    strips = 8
    strip = d // strips

    def res_slot(j, h=None):
        rows = pl.ds(pl.multiple_of(j * own_rows, own_rows), own_rows)
        if h is None:
            return res.at[rows, :]
        return res.at[rows, pl.ds(pl.multiple_of(h * strip, strip), strip)]

    def pair(s, ss, rs, i, dev):
        return remote(s, s, ss.at[i], rs.at[i], dev)

    def other(j):
        return j + 1 - 2 * core

    def res_to_n1(j, h):
        return pair(res_slot(j, h), r_ss, r_rs, h, to_n1)

    def res_on(j, h):
        return pair(res_slot(j, h), r_ss, r_rs, strips + h, to_n2)

    def res_to_n2(j):
        return pair(res_slot(j), r_ss, r_rs, 2 * strips, to_n2)

    def res_mate(j, i):
        return pair(res_slot(j), r_ss, r_rs, 2 * strips + 1 + i, to_mate)

    def att_slot(j, i):
        lanes = pl.ds(pl.multiple_of(j * HD, HD), HD)
        return att.at[i * ROWS_ATT : (i + 1) * ROWS_ATT, lanes]

    def att_to(j, i, which):
        return pair(att_slot(j, i), a_ss, a_rs, which * 4 + i, (to_n1, to_n2)[which])

    def att_on(j, i):
        return pair(att_slot(j, i), a_ss, a_rs, 8 + i, to_n2 if i < 2 else to_n1)

    def att_mate(j, i, which):
        return pair(att_slot(j, i), a_ss, a_rs, 12 + which * 4 + i, to_mate)

    def att_send(i):
        att_to(tp, i, 0).start()
        att_to(tp, i, 1).start()
        att_mate(tp, i, 0).start()

    def att_relay(i):
        att_to(n1, i, 0).wait_recv()
        att_to(n2, i, 1).wait_recv()
        att_on(n1 if i < 2 else n2, i).start()
        att_mate(n1, i, 1).start()
        att_mate(n2, i, 2).start()

    def att_diag(i):
        att_on(dg, i).wait_recv()
        att_mate(dg, i, 3).start()

    def att_taken(i):
        for which, j in enumerate((tp, n1, n2, dg)):
            att_mate(other(j), i, which).wait_recv()

    res_to_n2(tp).start()
    res_mate(tp, 0).start()

    gk = gate_ref.shape[1]
    ff = down_ref.shape[0]
    ff_pad = gu.shape[0] // 2

    def w_slot(which, b):
        if which == 2:
            return dw.at[pl.ds(pl.multiple_of(b * ff, ff), ff), :]
        lanes = pl.ds(pl.multiple_of(b * gk, gk), gk)
        row = (odd if which == 0 else 1 - odd) * ff_pad
        return gu.at[pl.ds(pl.multiple_of(row, ff_pad), ff), lanes]

    def w_copy(which, direction, t, late):
        s = w_slot(which, block_at(direction, t))
        return remote(
            s,
            s,
            w_ss.at[which // 2, direction, t],
            w_rs.at[which // 2, direction, t + late],
            (to_right, to_left)[direction],
        )

    def w_twin(which, direction, t):
        s = w_slot(which, block_at(direction, t))
        return remote(s, s, y_ss.at[direction, t], y_rs.at[direction, t], to_twin)

    def w_start(whiches):
        for which in whiches:
            for direction in range(2):
                w_copy(which, direction, 0, 1).start()

    @scoped("wstep")
    def w_step(whiches, t):
        for which in whiches:
            for direction in range(2):
                w_copy(which, direction, t, 0).wait_recv()

                @pl.when((t < half_n - 1) | (core == direction))
                def _():
                    w_copy(which, direction, t, 1).start()

                if which == 0:
                    w_twin(0, direction, t).start()

    @scoped("wlast")
    def w_last():
        for direction in range(2):

            @pl.when(core == direction)
            def _():
                w_copy(0, direction, half_n, 0).wait_recv()
                w_twin(0, direction, half_n).start()
                w_copy(2, direction, half_n, 0).wait_recv()

    @scoped("wtwin")
    def w_taken():
        def one(t, _):
            for direction in range(2):

                @pl.when((t < half_n) | (core == direction))
                def _():
                    w_twin(1, direction, t).wait_recv()

            return 0

        lax.fori_loop(1, half_n + 1, one, 0)

    def w_sent():
        def one(t, _):
            for direction in range(2):

                @pl.when((t < half_n - 1) | (core == direction))
                def _():
                    w_copy(0, direction, t, 1).wait_send()
                    w_copy(2, direction, t, 1).wait_send()

                @pl.when((t < half_n - 1) | (core == direction))
                def _():
                    w_twin(0, direction, t + 1).wait_send()

            return 0

        lax.fori_loop(0, half_n, one, 0)

    def prep_q(o, _):
        for u in range(TILES):
            i = o * TILES + u
            rows = pl.ds(pl.multiple_of(i * GRID_W, GRID_W), GRID_W)
            qrot[rows, :] = turned(q_ref[rows, :], qg_ref[...], i)
        return 0

    with jax.named_scope("prepq"):
        lax.fori_loop(0, grid_rows // TILES, prep_q, 0)
    own_lanes = pl.ds(pl.multiple_of(me * gk, gk), gk)
    gu[0:ff, own_lanes] = gate_ref[...]
    gu[ff_pad : ff_pad + ff, own_lanes] = up_ref[...]
    dw[pl.ds(pl.multiple_of(me * ff, ff), ff), :] = down_ref[...]
    for which in range(2):
        gu[which * ff_pad + ff : (which + 1) * ff_pad, :] = jnp.zeros((ff_pad - ff, gu.shape[1]), BF16)
    mx[...] = jnp.full(mx.shape, -1e30, F32)
    ls[...] = jnp.zeros(ls.shape, F32)
    acc[...] = jnp.zeros(acc.shape, F32)

    factor = HD ** (-0.5) * math.log2(math.e)

    dims = (((1,), (1,)), ((), ()))
    blocks = tok // ROWS_ATT

    def slabs(keys):
        return [(b, pl.ds(pl.multiple_of(h * slab, slab), slab)) for b, h in keys]

    def score(keys, i, s_ref, t_ref):
        q = qrot[i * ROWS_ATT : (i + 1) * ROWS_ATT, :]
        top = None
        for n_slab, (b, r) in enumerate(slabs(keys)):
            s = lax.dot_general(q, kv[b, r, 0:HD], dims, preferred_element_type=F32)
            s_ref[:, n_slab * slab : (n_slab + 1) * slab] = s
            for j in range(slab // HD):
                tile = s[:, j * HD : (j + 1) * HD]
                top = tile if top is None else jnp.maximum(top, tile)
        t_ref[...] = top

    def weigh(keys, i, s_ref, t_ref):
        rows = slice(i * ROWS_ATT, (i + 1) * ROWS_ATT)
        old = mx[rows, :]
        new = jnp.maximum(old, jnp.max(t_ref[...], axis=1, keepdims=True))
        mx[rows, :] = new
        alpha = jnp.exp2((old - new) * factor)
        base = new[:, 0:1]
        total = ls[rows, :] * alpha
        weighted = acc[rows, :] * alpha
        for n_slab, (b, r) in enumerate(slabs(keys)):
            raised = jnp.exp2((s_ref[:, n_slab * slab : (n_slab + 1) * slab] - base) * factor)
            for j in range(slab // HD):
                total = total + raised[:, j * HD : (j + 1) * HD]
            weighted = weighted + jnp.dot(
                raised.astype(BF16), kv[b, r, HD : 2 * HD], preferred_element_type=F32
            )
        ls[rows, :] = total
        acc[rows, :] = weighted

    held = ((sa, ta), (sb, tb))

    def attend_units(units, after=None):
        score(*units[0], *held[0])
        for u, unit in enumerate(units):
            if u + 1 < len(units):
                score(*units[u + 1], *held[(u + 1) % 2])
            weigh(*unit, *held[u % 2])
            if after is not None:
                after(u)

    def keys_of(t, a):
        return ((wrap(me - t), a), (wrap(me + t), a))

    @scoped("attend")
    def attend(keys):
        attend_units([(keys, i) for i in range(blocks)])

    @scoped("take")
    def kv_take(t, a):
        for which in (0, 2):
            for direction in range(2):
                kv_ring(direction, t, a, which, 0).wait_recv()

                @pl.when((t < half_n - 1) | (core == direction))
                def _():
                    kv_ring(direction, t, a, which, 1).start()

                if which == 0:
                    kv_near(direction, t, a, 0).start()
                kv_mate(direction, t, a, core, which).start()

    @scoped("near")
    def near_take(t, a):
        for direction in range(2):
            kv_near(direction, t, a, 1).wait_recv()
            kv_mate(direction, t, a, core, 1).start()

    @scoped("mate")
    def mate_take(t, a):
        for direction in range(2):
            for which in range(3):
                kv_mate(direction, t, a, 1 - core, which).wait_recv()

    def on_last(who, f):
        for direction in range(2):

            @pl.when(who == direction)
            def _():
                for a in range(2):
                    f(direction, a)

    attend(((me, 0), (me, 1)))
    kv_take(1, 0)
    kv_take(1, 1)
    w_start((0, 2))
    kv_take(2, 0)
    near_take(1, 0)

    def phase(p, _):
        kv_take((p + 1) // 2, lax.rem(p + 1, 2))

        @pl.when(p < 4 + strips)
        def _():
            res_to_n1(tp, p - 4).start()

        @pl.when(p >= 15 - strips)
        def _():
            res_to_n1(n1, p - 15 + strips).wait_recv()
            res_on(n1, p - 15 + strips).start()

        @pl.when(lax.rem(p, 3) == 1)
        def _():
            w_step((0,), p // 3)

        @pl.when(lax.rem(p, 3) == 2)
        def _():
            w_step((2,), p // 3)

        @pl.when(p == half_n)
        def _():
            res_to_n2(n2).wait_recv()
            res_mate(n2, 1).start()

        near_take((p - 1) // 2, lax.rem(p - 1, 2))
        tb, ab = (p - 2) // 2, lax.rem(p, 2)
        mate_take(tb, ab)
        attend(keys_of(tb, ab))
        return 0

    lax.fori_loop(4, 2 * half_n - 1, phase, 0)

    def last_take(direction, a):
        for which in (0, 2):
            kv_ring(direction, half_n, a, which, 0).wait_recv()
            if which == 0:
                kv_near(direction, half_n, a, 0).start()
            kv_mate(direction, half_n, a, core, which).start()

    def last_near(direction, a):
        kv_near(direction, half_n, a, 1).wait_recv()
        kv_mate(direction, half_n, a, core, 1).start()

    def last_mate(direction, a):
        for which in range(3):
            kv_mate(direction, half_n, a, 1 - core, which).wait_recv()

    with jax.named_scope("lasttake"):
        on_last(core, last_take)
    near_take(half_n - 1, 0)
    mate_take(half_n - 2, 1)
    attend(keys_of(half_n - 2, 1))
    near_take(half_n - 1, 1)
    w_step((0, 2), 5)
    mate_take(half_n - 1, 0)
    attend(keys_of(half_n - 1, 0))
    with jax.named_scope("lastnear"):
        on_last(core, last_near)
    mate_take(half_n - 1, 1)
    res_mate(n1, 2).start()
    with jax.named_scope("lastmate"):
        on_last(1 - core, last_mate)

    def finish(u):
        if u % 2 == 0:
            return
        i = u // 2
        rows = slice(i * ROWS_ATT, (i + 1) * ROWS_ATT)
        below = jnp.sum(ls[rows, :], axis=1, keepdims=True)
        att[rows, pl.ds(pl.multiple_of(tp * HD, HD), HD)] = (acc[rows, :] / below).astype(BF16)
        if i > 0:
            att_send(i - 1)
        if i == 1:
            w_step((0, 2), 6)

    last_keys = (keys_of(half_n - 1, 1), ((wrap(me + half_n), 0), (wrap(me + half_n), 1)))
    with jax.named_scope("lastattend"):
        attend_units([(last_keys[u % 2], u // 2) for u in range(2 * blocks)], finish)
    att_send(blocks - 1)
    load_ow.wait()
    with jax.named_scope("relay"):
        for i in range(blocks):
            att_relay(i)
    w_step((0, 2), 7)
    with jax.named_scope("diag"):
        for i in range(blocks):
            att_diag(i)
    with jax.named_scope("taken"):
        for i in range(blocks):
            att_taken(i)
        res_mate(other(tp), 0).wait_recv()
        res_mate(other(n2), 1).wait_recv()

    def project(o, _):
        i = jnp.where(o == 0, x, jnp.where(o == 1, n2x, jnp.where(o == 2, n1x, dgx)))

        @pl.when(o == 1)
        def _():
            for h in range(strips):
                res_on(dg, h).wait_recv()
            res_mate(dg, 3).start()
            w_last()

        @pl.when(o == 2)
        def _():
            res_mate(other(n1), 2).wait_recv()

        @pl.when(o == 3)
        def _():
            res_mate(other(dg), 3).wait_recv()

        rows = pl.ds(pl.multiple_of(i * ROWS_FF, ROWS_FF), ROWS_FF)
        middle = res[rows, :].astype(F32) + jnp.dot(
            att[rows, :], ow[...], preferred_element_type=F32
        )
        scale = lax.rsqrt(jnp.mean(middle * middle, axis=-1, keepdims=True) + 1e-06)
        nrm[rows, :] = (middle * scale * ng_ref[...]).astype(BF16)
        for j in range(2):

            @pl.when((o == 0) & (core == j))
            def _():
                mid[...] = middle[j * own_rows : (j + 1) * own_rows, :]

        return 0

    with jax.named_scope("project"):
        lax.fori_loop(0, tok // ROWS_FF, project, 0)
    w_taken()

    def units(i, _):
        rows = pl.ds(pl.multiple_of(i * ROWS_FF, ROWS_FF), ROWS_FF)
        n_rows = nrm[rows, :]
        act = lax.dot_general(n_rows, gu[...], dims, preferred_element_type=F32)
        gate = act[:, 0:ff]
        hid[rows, :] = (gate / (1.0 + jnp.exp(-gate)) * act[:, ff_pad : ff_pad + ff]).astype(BF16)

        return 0

    with jax.named_scope("units"):
        lax.fori_loop(0, tok // ROWS_FF, units, 0)

    near = (n1x, n2x)
    far = (n2x, n1x)
    to_near = (to_n1, to_n2)
    to_far = (to_n2, to_n1)

    def col_block(g, k):
        return wrap(me - k) if g == 0 else wrap(me + k + 1)

    def d2_copy(g, k):
        return remote(d2s.at[g, k], d2r.at[g, k], t_ss.at[0, g, k], t_rs.at[0, g, k], to_mate)

    def s1_copy(g, k):
        return remote(s1s.at[g, k], s1r.at[g, k], t_ss.at[1, g, k], t_rs.at[1, g, k], to_near[g])

    def s2_copy(g, k):
        return remote(s2s.at[g, k], s2r.at[g, k], t_ss.at[2, g, k], t_rs.at[2, g, k], to_far[g])

    @scoped("stage0")
    def stage0(k):
        for g in range(2):
            b = col_block(g, k)
            part[...] = jnp.dot(
                hid[...],
                dw[pl.ds(pl.multiple_of(b * ff, ff), ff), :],
                preferred_element_type=F32,
            )
            for c in range(4):
                rows = slice(c * own_rows, (c + 1) * own_rows)
                theirs = pl.ds(pl.multiple_of((c * 2 + 1 - core) * own_rows, own_rows), own_rows)
                mine = pl.ds(pl.multiple_of((c * 2 + core) * own_rows, own_rows), own_rows)
                d2s[g, k, rows, :] = part[theirs, :].astype(BF16)
                kept[g, k, rows, :] = part[mine, :]
            d2_copy(g, k).start()

    @scoped("stage1")
    def stage1(k):
        for g in range(2):
            d2_copy(g, k).wait_recv()

            def summed(c):
                at = pl.ds(pl.multiple_of(c * own_rows, own_rows), own_rows)
                return kept[g, k, at, :] + d2r[g, k, at, :].astype(F32)

            s1s[g, k, 0:own_rows, :] = summed(near[g]).astype(BF16)
            s1s[g, k, own_rows : 2 * own_rows, :] = summed(dgx).astype(BF16)
            yk[g, k, 0] = summed(x)
            yk[g, k, 1] = summed(far[g])
            s1_copy(g, k).start()

    @scoped("stage2")
    def stage2(k):
        for g in range(2):
            s1_copy(g, k).wait_recv()
            s2s[g, k] = (
                yk[g, k, 1] + s1r[g, k, own_rows : 2 * own_rows, :].astype(F32)
            ).astype(BF16)
            zk[g, k] = yk[g, k, 0] + s1r[g, k, 0:own_rows, :].astype(F32)
            s2_copy(g, k).start()

    @scoped("stage3")
    def stage3(k):
        for g in range(2):
            s2_copy(g, k).wait_recv()
            lanes = pl.ds(pl.multiple_of(col_block(g, k) * HD, HD), HD)
            out_ref[:, lanes] = (mid[:, lanes] + zk[g, k] + s2r[g, k].astype(F32)).astype(BF16)

    lag = 2

    def columns(k, _):
        @pl.when(k < half_n)
        def _():
            stage0(k)

        @pl.when(k >= lag)
        def _():
            stage1(k - lag)

        return 0

    lax.fori_loop(0, half_n + lag, columns, 0)

    def sums(k, _):
        @pl.when(k < half_n)
        def _():
            stage2(k)

        @pl.when(k >= lag)
        def _():
            stage3(k - lag)

        return 0

    lax.fori_loop(0, half_n + lag, sums, 0)

    def kv_sent(t, _):
        for a in range(2):
            for direction in range(2):
                for which in (0, 2):

                    @pl.when((t < half_n - 1) | (core == direction))
                    def _():
                        kv_ring(direction, t, a, which, 1).wait_send()

                @pl.when(t > 0)
                def _():
                    kv_near(direction, t, a, 0).wait_send()
                    for which in range(3):
                        kv_mate(direction, t, a, core, which).wait_send()

        return 0

    lax.fori_loop(0, half_n, kv_sent, 0)

    def last_sent(direction, a):
        kv_near(direction, half_n, a, 0).wait_send()
        for which in range(3):
            kv_mate(direction, half_n, a, core, which).wait_send()

    on_last(core, last_sent)
    w_sent()
    for h in range(strips):
        res_to_n1(tp, h).wait_send()
        res_on(n1, h).wait_send()
    res_to_n2(tp).wait_send()
    for i, j in enumerate((tp, n2, n1, dg)):
        res_mate(j, i).wait_send()
    for i in range(blocks):
        att_to(tp, i, 0).wait_send()
        att_to(tp, i, 1).wait_send()
        att_on(n1 if i < 2 else n2, i).wait_send()
        for which, j in enumerate((tp, n1, n2, dg)):
            att_mate(j, i, which).wait_send()

    def sums_sent(k, _):
        for g in range(2):
            d2_copy(g, k).wait_send()
            s1_copy(g, k).wait_send()
            s2_copy(g, k).wait_send()
        return 0

    lax.fori_loop(0, half_n, sums_sent, 0)


def local(
    n,
    n_tp,
    queries,
    keys,
    values,
    query_gain,
    key_gain,
    out_weight,
    residual_in,
    norm_gain,
    gate_weight,
    up_weight,
    down_weight,
):
    tok = queries.shape[0]
    own_rows, d = residual_in.shape
    ff = down_weight.shape[0]
    gk = gate_weight.shape[0]
    ff_pad = -(-ff // HD) * HD
    half = HD // 2
    half_n = n // 2
    inverse = 10000.0 ** (-np.arange(0, half, 2, dtype=np.float32) / half)
    inverse = jnp.asarray(np.tile(np.repeat(inverse, 2), 2)[None].astype(np.float32))
    vmem = pl.BlockSpec(memory_space=pltpu.VMEM)
    dma = pltpu.SemaphoreType.DMA
    scratch = [
        pltpu.VMEM((n, tok, 2 * HD), BF16),
        pltpu.VMEM((tok, HD), BF16),
        pltpu.VMEM((tok, HD), F32),
        pltpu.VMEM((tok, HD), F32),
        pltpu.VMEM((tok, HD), F32),
        pltpu.VMEM((ROWS_ATT, tok), F32),
        pltpu.VMEM((ROWS_ATT, tok), F32),
        pltpu.VMEM((ROWS_ATT, HD), F32),
        pltpu.VMEM((ROWS_ATT, HD), F32),
        pltpu.VMEM((tok // GRID_W, HD), F32),
        pltpu.VMEM((tok // GRID_W, HD), F32),
        pltpu.VMEM((2 * ff_pad, n * gk), BF16),
        pltpu.VMEM((n * ff, HD), BF16),
        pltpu.VMEM(out_weight.shape, BF16),
        pltpu.VMEM((tok, d), BF16),
        pltpu.VMEM((tok, HQ * HD), BF16),
        pltpu.VMEM((tok, d), BF16),
        pltpu.VMEM((own_rows, d), F32),
        pltpu.VMEM((tok, ff), BF16),
        pltpu.VMEM((tok, HD), F32),
        pltpu.VMEM((2, half_n, tok // 2, HD), F32),
        pltpu.VMEM((2, half_n, tok // 2, HD), BF16),
        pltpu.VMEM((2, half_n, tok // 2, HD), BF16),
        pltpu.VMEM((2, half_n, 2 * own_rows, HD), BF16),
        pltpu.VMEM((2, half_n, 2 * own_rows, HD), BF16),
        pltpu.VMEM((2, half_n, own_rows, HD), BF16),
        pltpu.VMEM((2, half_n, own_rows, HD), BF16),
        pltpu.VMEM((2, half_n, 2, own_rows, HD), F32),
        pltpu.VMEM((2, half_n, own_rows, HD), F32),
        dma,
        dma((2, half_n + 1, 2, 2)),
        dma((2, half_n + 1, 2, 2)),
        dma((2, half_n + 1, 2)),
        dma((2, half_n + 1, 2)),
        dma((2, half_n + 1, 2, 3)),
        dma((2, half_n + 1, 2, 3)),
        dma((2, 2, half_n + 1)),
        dma((2, 2, half_n + 1)),
        dma((2, half_n + 1)),
        dma((2, half_n + 1)),
        dma((28,)),
        dma((28,)),
        dma((21,)),
        dma((21,)),
        dma((3, 2, half_n)),
        dma((3, 2, half_n)),
    ]
    specs = [vmem] * 12
    specs[6] = pl.BlockSpec(memory_space=pl.ANY)
    return pl.pallas_call(
        functools.partial(layer_kernel, n, n_tp),
        out_shape=jax.ShapeDtypeStruct((own_rows, d), BF16),
        in_specs=specs,
        out_specs=vmem,
        scratch_shapes=scratch,
        compiler_params=pltpu.CompilerParams(
            collective_id=0, has_side_effects=True, vmem_limit_bytes=67043328
        ),
        name="layer",
    )(
        queries,
        keys,
        values,
        query_gain[None],
        key_gain[None],
        inverse,
        out_weight,
        residual_in,
        norm_gain[None],
        gate_weight.T,
        up_weight.T,
        down_weight,
    )


def solution(mesh):
    placed = (
        P(("grp", "sp"), "tp"),
        P(("grp", "sp"), None),
        P(("grp", "sp"), None),
        P(),
        P(),
        P(),
        P(("grp", "sp", "tp"), None),
        P(),
        P("sp", "tp"),
        P("sp", "tp"),
        P("tp", "sp"),
    )
    return jax.shard_map(
        functools.partial(local, mesh.shape["sp"], mesh.shape["tp"]),
        mesh=mesh,
        in_specs=placed,
        out_specs=P(("grp", "sp", "tp"), None),
        check_vma=False,
    )
```

```python
import functools
import math

import jax
import jax.numpy as jnp
import numpy as np
from jax import lax
from jax.experimental import pallas as pl
from jax.experimental.pallas import tpu as pltpu
from jax.sharding import PartitionSpec as P

HQ = 8
KV = 2
HD = 128
GRID_W = 64
MESH = pl.DeviceIdType.MESH
F32 = jnp.float32
BF16 = jnp.bfloat16
ROWS_ATT = 256
ROWS_FF = 256
TILES = 4


def scoped(name):
    def wrapped(f):
        def call(*args):
            with jax.named_scope(name):
                return f(*args)

        return call

    return wrapped


def layer_kernel(
    n,
    n_tp,
    q_ref,
    k_ref,
    v_ref,
    qg_ref,
    kg_ref,
    inv_ref,
    ow_hbm,
    res_ref,
    ng_ref,
    gate_ref,
    up_ref,
    down_ref,
    out_ref,
    kv,
    qrot,
    acc,
    mx,
    ls,
    sa,
    sb,
    ta,
    tb,
    cosr,
    sinr,
    gu,
    dw,
    ow,
    res,
    att,
    nrm,
    mid,
    hid,
    part,
    d2s,
    d2r,
    yk,
    xs,
    xr,
    ow_sem,
    kv_ss,
    kv_rs,
    kx_rs,
    kd_rs,
    w_ss,
    w_rs,
    y_rs,
    a_ss,
    a_rs,
    r_ss,
    r_rs,
    t_ss,
    t_rs,
):
    me = lax.axis_index("sp")
    tp = lax.axis_index("tp")
    grp = lax.axis_index("grp")
    odd = lax.rem(grp, 2)
    core = lax.rem(tp, 2)
    x = tp // 2
    tok = q_ref.shape[0]
    d = res_ref.shape[1]
    own_rows = res_ref.shape[0]
    half_n = n // 2
    kv_head = tp // (n_tp // KV)

    def wrap(i):
        return lax.rem(i + n, n)

    right = wrap(me + 1)
    left = wrap(me - 1)
    n1x = x + 1 - 2 * lax.rem(x, 2)
    n2x = 3 - x
    dgx = 3 - n1x
    mate = x * 2 + 1 - core
    n1 = n1x * 2 + core
    n2 = n2x * 2 + core
    dg = dgx * 2 + core
    to_right, to_left = {"sp": right}, {"sp": left}
    to_mate, to_n1, to_n2 = {"tp": mate}, {"tp": n1}, {"tp": n2}
    to_twin = {"grp": grp + 1 - 2 * odd}

    def remote(src, dst, ss, rs, dev):
        return pltpu.make_async_remote_copy(
            src_ref=src, dst_ref=dst, send_sem=ss, recv_sem=rs, device_id=dev, device_id_type=MESH
        )

    def arrived(span, sem):
        pltpu.make_async_copy(span, span, sem).wait()

    load_ow = pltpu.make_async_copy(ow_hbm, ow, ow_sem)
    load_ow.start()

    barrier = pltpu.get_barrier_semaphore()
    for dev in (to_right, to_left, to_mate, to_n1, to_n2, to_twin):
        pl.semaphore_signal(barrier, inc=1, device_id=dev, device_id_type=MESH)

    grid_rows = tok // GRID_W
    lane = lax.broadcasted_iota(jnp.int32, (GRID_W, HD), 1)
    row_pos = (me * grid_rows + lax.broadcasted_iota(jnp.int32, (grid_rows, HD), 0)).astype(F32)
    row_ang = row_pos * inv_ref[...]
    cosr[...] = jnp.cos(row_ang)
    sinr[...] = jnp.sin(row_ang)
    col_ang = lax.broadcasted_iota(jnp.int32, (GRID_W, HD), 0).astype(F32) * inv_ref[...]
    cos_col = jnp.cos(col_ang)
    sin_col = jnp.sin(col_ang)
    even = lax.rem(lane, 2) == 0
    by_row = lane < HD // 2

    def turned(source, gain, i):
        v = source.astype(F32)
        v = v * lax.rsqrt(jnp.mean(v * v, axis=-1, keepdims=True) + 1e-06) * gain
        cosine = jnp.where(by_row, cosr[pl.ds(i, 1), :], cos_col)
        sine = jnp.where(by_row, sinr[pl.ds(i, 1), :], sin_col)
        swapped = jnp.where(even, pltpu.roll(v, HD - 1, 1), pltpu.roll(v, 1, 1))
        signed = jnp.where(even, -sine, sine)
        return (v * cosine + swapped * signed).astype(BF16)

    kv_lanes = pl.ds(pl.multiple_of(kv_head * HD, HD), HD)

    def prep_k(o, _):
        for u in range(TILES):
            i = o * TILES + u
            rows = pl.ds(pl.multiple_of(i * GRID_W, GRID_W), GRID_W)
            kv[me, rows, 0:HD] = turned(k_ref[rows, kv_lanes], kg_ref[...], i)
            kv[me, rows, HD : 2 * HD] = v_ref[rows, kv_lanes]
        return 0

    with jax.named_scope("prepk"):
        lax.fori_loop(0, grid_rows // TILES, prep_k, 0)
        res[pl.ds(pl.multiple_of(tp * own_rows, own_rows), own_rows), :] = res_ref[...]
    with jax.named_scope("barrier"):
        pl.semaphore_wait(barrier, 6)

    quarter = tok // 4
    slab = tok // 2

    side = lax.rem(x, 2)
    share = quarter * 5 // 16
    sizes = (share, share, quarter - 2 * share)

    def block_at(direction, t):
        return wrap(me - t) if direction == 0 else wrap(me + t)

    def piece(direction, t, a, c, which):
        start = (side * share, (1 - side) * share, 2 * share)[which]
        at = pl.multiple_of((2 * a + c) * quarter + start, 16)
        return kv.at[block_at(direction, t), pl.ds(at, sizes[which]), :]

    def kv_ring(direction, t, a, which, late):
        s = piece(direction, t, a, core, which)
        return remote(
            s,
            s,
            kv_ss.at[t],
            kv_rs.at[t + late, a, which // 2],
            (to_right, to_left)[direction],
        )

    def kv_near(direction, t, a, which):
        s = piece(direction, t, a, core, which)
        return remote(s, s, kv_ss.at[t], kx_rs.at[t, a], to_n1)

    def kv_mate(direction, t, a, c, which):
        s = piece(direction, t, a, c, which)
        return remote(s, s, kv_ss.at[t], kd_rs.at[t, a], to_mate)

    def kv_span(rows):
        return kv.at[0, 0:rows]

    for a in range(2):
        for which in (0, 2):
            for direction in range(2):
                kv_ring(direction, 0, a, which, 1).start()

    strips = 8
    strip = d // strips

    def res_slot(j, h=None):
        rows = pl.ds(pl.multiple_of(j * own_rows, own_rows), own_rows)
        if h is None:
            return res.at[rows, :]
        return res.at[rows, pl.ds(pl.multiple_of(h * strip, strip), strip)]

    def pair(s, ss, rs, i, dev):
        return remote(s, s, ss, rs.at[i], dev)

    def other(j):
        return j + 1 - 2 * core

    def res_to_n1(j, h):
        return pair(res_slot(j, h), r_ss, r_rs, h, to_n1)

    def res_on(j, h):
        return pair(res_slot(j, h), r_ss, r_rs, strips, to_n2)

    def res_to_n2(j):
        return pair(res_slot(j), r_ss, r_rs, strips + 1, to_n2)

    def res_mate(j, i):
        return pair(res_slot(j), r_ss, r_rs, strips + 2, to_mate)

    def att_slot(j, i):
        lanes = pl.ds(pl.multiple_of(j * HD, HD), HD)
        return att.at[i * ROWS_ATT : (i + 1) * ROWS_ATT, lanes]

    def att_to(j, i, which):
        return pair(att_slot(j, i), a_ss, a_rs, i, (to_n1, to_n2)[which])

    def att_on(j, i):
        return pair(att_slot(j, i), a_ss, a_rs, 4 + i, to_n2 if i < 2 else to_n1)

    def att_mate(j, i, which):
        return pair(att_slot(j, i), a_ss, a_rs, 8 + i, to_mate)

    def att_send(i):
        att_to(tp, i, 0).start()
        att_to(tp, i, 1).start()
        att_mate(tp, i, 0).start()

    def att_relay(i):
        arrived(att.at[0:ROWS_ATT, 0 : 2 * HD], a_rs.at[i])
        att_on(n1 if i < 2 else n2, i).start()
        att_mate(n1, i, 1).start()
        att_mate(n2, i, 2).start()

    def att_diag(i):
        att_on(dg, i).wait_recv()
        att_mate(dg, i, 3).start()

    def att_taken(i):
        arrived(att.at[0:ROWS_ATT, 0 : 4 * HD], a_rs.at[8 + i])

    def res_pass(h):
        res_to_n1(n1, h).wait_recv()
        res_on(n1, h).start()

    res_to_n2(tp).start()
    res_mate(tp, 0).start()

    gk = gate_ref.shape[1]
    ff = down_ref.shape[0]
    ff_pad = gu.shape[0] // 2

    def w_slot(which, b):
        if which == 2:
            return dw.at[:, pl.ds(pl.multiple_of(b * HD, HD), HD)]
        lanes = pl.ds(pl.multiple_of(b * gk, gk), gk)
        row = (odd if which == 0 else 1 - odd) * ff_pad
        return gu.at[pl.ds(pl.multiple_of(row, ff_pad), ff), lanes]

    def w_copy(which, direction, t, late):
        s = w_slot(which, block_at(direction, t))
        return remote(
            s,
            s,
            w_ss.at[which // 2, t],
            w_rs.at[which // 2, t + late],
            (to_right, to_left)[direction],
        )

    def w_twin(which, direction, t):
        s = w_slot(which, block_at(direction, t))
        return remote(s, s, w_ss.at[0, t], y_rs, to_twin)

    def w_span(which, count):
        return (gu, None, dw)[which].at[0:ff, 0 : count * gk]

    def w_start(whiches):
        for which in whiches:
            for direction in range(2):
                w_copy(which, direction, 0, 1).start()

    @scoped("wstep")
    def w_step(whiches, t):
        for which in whiches:
            arrived(w_span(which, 2), w_rs.at[which // 2, t])
            for direction in range(2):

                @pl.when((t < half_n - 1) | (core == direction))
                def _():
                    w_copy(which, direction, t, 1).start()

                if which == 0:
                    w_twin(0, direction, t).start()

    def w_last(which):
        for direction in range(2):

            @pl.when(core == direction)
            def _():
                arrived(w_span(which, 1), w_rs.at[which // 2, half_n])
                if which == 0:
                    w_twin(0, direction, half_n).start()

    w_order = [(2, 2)]
    for t in range(4, half_n + 1):
        w_order += [(0, t), (2, t - 1)]
    w_order += [(2, half_n)]

    @scoped("pump")
    def pump(count=1):
        for _ in range(count):
            which, t = w_order.pop(0)
            if t < half_n:
                w_step((which,), t)
            else:
                w_last(which)

    @scoped("wtwin")
    def w_taken():
        arrived(w_span(0, n - 1), y_rs)

    def w_sent():
        for t in range(half_n + 1):
            ring = 2 if t < half_n - 1 else half_n - t
            twin = 0 if t == 0 else 2 if t < half_n else 1
            arrived(w_span(0, ring + twin), w_ss.at[0, t])
            if ring > 0:
                arrived(w_span(2, ring), w_ss.at[1, t])

    def prep_q(o, _):
        for u in range(TILES):
            i = o * TILES + u
            rows = pl.ds(pl.multiple_of(i * GRID_W, GRID_W), GRID_W)
            qrot[rows, :] = turned(q_ref[rows, :], qg_ref[...], i)
        return 0

    with jax.named_scope("prepq"):
        lax.fori_loop(0, grid_rows // TILES, prep_q, 0)
    own_lanes = pl.ds(pl.multiple_of(me * gk, gk), gk)
    gu[0:ff, own_lanes] = gate_ref[...]
    gu[ff_pad : ff_pad + ff, own_lanes] = up_ref[...]
    dw[:, pl.ds(pl.multiple_of(me * HD, HD), HD)] = down_ref[...]
    for which in range(2):
        gu[which * ff_pad + ff : (which + 1) * ff_pad, :] = jnp.zeros((ff_pad - ff, gu.shape[1]), BF16)
    mx[...] = jnp.full(mx.shape, -1e30, F32)
    ls[...] = jnp.zeros(ls.shape, F32)
    acc[...] = jnp.zeros(acc.shape, F32)

    factor = HD ** (-0.5) * math.log2(math.e)

    dims = (((1,), (1,)), ((), ()))
    blocks = tok // ROWS_ATT

    def slabs(keys):
        return [(b, pl.ds(pl.multiple_of(h * slab, slab), slab)) for b, h in keys]

    def score(keys, i, s_ref, t_ref):
        q = qrot[i * ROWS_ATT : (i + 1) * ROWS_ATT, :]
        top = None
        for n_slab, (b, r) in enumerate(slabs(keys)):
            s = lax.dot_general(q, kv[b, r, 0:HD], dims, preferred_element_type=F32)
            s_ref[:, n_slab * slab : (n_slab + 1) * slab] = s
            for j in range(slab // HD):
                tile = s[:, j * HD : (j + 1) * HD]
                top = tile if top is None else jnp.maximum(top, tile)
        t_ref[...] = top

    def weigh(keys, i, s_ref, t_ref):
        rows = slice(i * ROWS_ATT, (i + 1) * ROWS_ATT)
        old = mx[rows, :]
        new = jnp.maximum(old, jnp.max(t_ref[...], axis=1, keepdims=True))
        mx[rows, :] = new
        alpha = jnp.exp2((old - new) * factor)
        base = new[:, 0:1]
        total = ls[rows, :] * alpha
        weighted = acc[rows, :] * alpha
        for n_slab, (b, r) in enumerate(slabs(keys)):
            raised = jnp.exp2((s_ref[:, n_slab * slab : (n_slab + 1) * slab] - base) * factor)
            for j in range(slab // HD):
                total = total + raised[:, j * HD : (j + 1) * HD]
            weighted = weighted + jnp.dot(
                raised.astype(BF16), kv[b, r, HD : 2 * HD], preferred_element_type=F32
            )
        ls[rows, :] = total
        acc[rows, :] = weighted

    held = ((sa, ta), (sb, tb))

    def attend_units(units, after=None):
        score(*units[0], *held[0])
        for u, unit in enumerate(units):
            if u + 1 < len(units):
                score(*units[u + 1], *held[(u + 1) % 2])
            weigh(*unit, *held[u % 2])
            if after is not None:
                after(u)

    def keys_of(t, a):
        return ((wrap(me - t), a), (wrap(me + t), a))

    @scoped("attend")
    def attend(keys):
        attend_units([(keys, i) for i in range(blocks)])

    @scoped("take")
    def kv_take(t, a):
        for which in (0, 2):
            arrived(kv_span(2 * sizes[which]), kv_rs.at[t, a, which // 2])
            for direction in range(2):

                @pl.when((t < half_n - 1) | (core == direction))
                def _():
                    kv_ring(direction, t, a, which, 1).start()

                if which == 0:
                    kv_near(direction, t, a, 0).start()
                kv_mate(direction, t, a, core, which).start()

    @scoped("near")
    def near_take(t, a):
        arrived(kv_span(2 * share), kx_rs.at[t, a])
        for direction in range(2):
            kv_mate(direction, t, a, core, 1).start()

    @scoped("mate")
    def mate_take(t, a):
        arrived(kv_span(2 * quarter), kd_rs.at[t, a])

    def on_last(who, f):
        for direction in range(2):

            @pl.when(who == direction)
            def _():
                for a in range(2):
                    f(direction, a)

    attend(((me, 0), (me, 1)))
    kv_take(1, 0)
    kv_take(1, 1)
    kv_take(2, 0)
    near_take(1, 0)

    def phase(p, _):
        kv_take((p + 1) // 2, lax.rem(p + 1, 2))

        @pl.when(p < 8)
        def _():
            res_to_n1(tp, p - 4).start()

        @pl.when((lax.rem(p, 2) == 0) & (p >= 8))
        def _():
            res_to_n1(tp, p // 2).start()

        @pl.when(p >= 8)
        def _():
            res_pass(p - 8)

        @pl.when(p == 8)
        def _():
            w_start((0,))

        @pl.when((lax.rem(p, 2) == 0) & (p >= 10))
        def _():
            w_step((0,), (p - 8) // 2)

        @pl.when(p == 9)
        def _():
            w_start((2,))

        @pl.when(p == 13)
        def _():
            w_step((2,), 1)

        @pl.when(p == half_n)
        def _():
            res_to_n2(n2).wait_recv()
            res_mate(n2, 1).start()

        near_take((p - 1) // 2, lax.rem(p - 1, 2))
        tb, ab = (p - 2) // 2, lax.rem(p, 2)
        mate_take(tb, ab)
        attend(keys_of(tb, ab))
        return 0

    lax.fori_loop(4, 2 * half_n - 1, phase, 0)

    def last_take(direction, a):
        for which in (0, 2):
            arrived(kv_span(sizes[which]), kv_rs.at[half_n, a, which // 2])
            if which == 0:
                kv_near(direction, half_n, a, 0).start()
            kv_mate(direction, half_n, a, core, which).start()

    def last_near(direction, a):
        arrived(kv_span(share), kx_rs.at[half_n, a])
        kv_mate(direction, half_n, a, core, 1).start()

    def last_mate(direction, a):
        arrived(kv_span(quarter), kd_rs.at[half_n, a])

    with jax.named_scope("lasttake"):
        on_last(core, last_take)
    near_take(half_n - 1, 0)
    mate_take(half_n - 2, 1)
    near_take(half_n - 1, 1)
    mate_take(half_n - 1, 0)
    pump()
    relay, diag, taken = scoped("relay")(att_relay), scoped("diag")(att_diag), scoped("taken")(att_taken)

    last_keys = (
        keys_of(half_n - 2, 1),
        keys_of(half_n - 1, 0),
        keys_of(half_n - 1, 1),
        ((wrap(me + half_n), 0), (wrap(me + half_n), 1)),
    )
    order = [(0, 0), (1, 0), (2, 0), (0, 1), (3, 0), (1, 1), (2, 1), (3, 1)]
    order += [(g, i) for i in range(2, blocks) for g in range(4)]

    def finish(u):
        if u == 0:
            mate_take(half_n - 1, 1)
        if u == 1:
            with jax.named_scope("lastnear"):
                on_last(core, last_near)
            res_pass(7)
            res_mate(n1, 2).start()
        if u == 2:
            with jax.named_scope("lastmate"):
                on_last(1 - core, last_mate)
        if u > 0 and order[u - 1][0] == 3:
            att_send(order[u - 1][1])
        g, i = order[u]
        if g != 3:
            return
        rows = slice(i * ROWS_ATT, (i + 1) * ROWS_ATT)
        below = jnp.sum(ls[rows, :], axis=1, keepdims=True)
        att[rows, pl.ds(pl.multiple_of(tp * HD, HD), HD)] = (acc[rows, :] / below).astype(BF16)
        pump()
        if i == 2:
            relay(0)

    with jax.named_scope("lastattend"):
        attend_units([(last_keys[g], i) for g, i in order], finish)
    att_send(blocks - 1)
    with jax.named_scope("resdiag"):
        arrived(res.at[0:own_rows], r_rs.at[strips])
        res_mate(dg, 3).start()
    load_ow.wait()

    @scoped("project")
    def project(i):
        rows = slice(i * ROWS_FF, (i + 1) * ROWS_FF)
        middle = res[rows, :].astype(F32) + jnp.dot(
            att[rows, :], ow[...], preferred_element_type=F32
        )
        scale = lax.rsqrt(jnp.mean(middle * middle, axis=-1, keepdims=True) + 1e-06)
        nrm[rows, :] = (middle * scale * ng_ref[...]).astype(BF16)
        for j in range(2):

            @pl.when(tp == 2 * i + j)
            def _():
                mid[...] = middle[j * own_rows : (j + 1) * own_rows, :]

    relay(1)
    pump()
    diag(0)
    relay(2)
    pump()
    with jax.named_scope("resmate"):
        arrived(res.at[0 : 4 * own_rows], r_rs.at[strips + 2])
    taken(0)
    project(0)
    relay(3)
    diag(1)
    pump()
    taken(1)
    project(1)
    diag(2)
    pump()
    taken(2)
    project(2)
    diag(3)
    pump()
    taken(3)
    project(3)
    w_taken()

    half_d = d // 2
    cols = (slice(0, half_d), slice(half_d, d))
    owners = (dgx, n1x, n2x, x)

    def d2_copy(o):
        return remote(d2s.at[o], d2r.at[o], t_ss, t_rs.at[o], to_mate)

    def x_copy(m):
        dev = (to_n1, to_n2, to_n1, to_n1, to_n2, to_n2)[m]
        return remote(xs.at[m], xr.at[m], t_ss, t_rs.at[4 + m], dev)

    @scoped("units")
    def units(o):
        rows = pl.ds(pl.multiple_of(owners[o] * ROWS_FF, ROWS_FF), ROWS_FF)
        act = lax.dot_general(nrm[rows, :], gu[...], dims, preferred_element_type=F32)
        gate = act[:, 0:ff]
        hid[o] = (gate / (1.0 + jnp.exp(-gate)) * act[:, ff_pad : ff_pad + ff]).astype(BF16)

    @scoped("block")
    def block(o):
        part[...] = jnp.dot(hid[o], dw[...], preferred_element_type=F32)
        theirs = pl.ds(pl.multiple_of((1 - core) * own_rows, own_rows), own_rows)
        mine = pl.ds(pl.multiple_of(core * own_rows, own_rows), own_rows)
        d2s[o] = part[theirs, :].astype(BF16)
        yk[o] = part[mine, :]
        d2_copy(o).start()

    def both(o, c):
        return yk[o, :, cols[c]] + d2r[o, :, cols[c]].astype(F32)

    @scoped("sums")
    def sums(o):
        d2_copy(o).wait_recv()
        if o == 0:
            for c in range(2):
                xs[c] = both(0, c).astype(BF16)
                x_copy(c).start()
        elif o == 1:
            xs[2] = both(1, 0).astype(BF16)
            x_copy(2).start()
            yk[1, :, cols[1]] = both(1, 1)
        elif o == 2:
            xs[4] = both(2, 1).astype(BF16)
            x_copy(4).start()
            yk[2, :, cols[0]] = both(2, 0)
        else:
            for c in range(2):
                yk[3, :, cols[c]] = both(3, c) + mid[:, cols[c]]

    units(0)
    pump()
    units(1)
    units(2)
    pump()
    units(3)
    pump(len(w_order))
    block(0)
    sums(0)
    block(1)
    block(2)
    sums(1)
    block(3)
    sums(2)
    sums(3)
    with jax.named_scope("pass"):
        x_copy(1).wait_recv()
        xs[3] = (yk[1, :, cols[1]] + xr[1].astype(F32)).astype(BF16)
        x_copy(3).start()
        x_copy(0).wait_recv()
        xs[5] = (yk[2, :, cols[0]] + xr[0].astype(F32)).astype(BF16)
        x_copy(5).start()
    for t in range(half_n + 1):
        ring = (2 if t < half_n - 1 else half_n - t) * 2 * (quarter - share)
        others = 0 if t == 0 else (2 if t < half_n else 1) * 2 * (share + quarter)
        arrived(kv.at[0:2, 0 : (ring + others) // 2], kv_ss.at[t])
    w_sent()
    arrived(res.at[0 : 7 * own_rows], r_ss)
    arrived(att.at[:, 0 : 7 * HD], a_ss)
    with jax.named_scope("final"):
        for c, (m1, m2) in enumerate(((2, 5), (4, 3))):
            x_copy(m1).wait_recv()
            x_copy(m2).wait_recv()
            out_ref[:, cols[c]] = (
                yk[3, :, cols[c]] + xr[m1].astype(F32) + xr[m2].astype(F32)
            ).astype(BF16)

    arrived(res.at[0 : 7 * own_rows], t_ss)


def local(
    n,
    n_tp,
    queries,
    keys,
    values,
    query_gain,
    key_gain,
    out_weight,
    residual_in,
    norm_gain,
    gate_weight,
    up_weight,
    down_weight,
):
    tok = queries.shape[0]
    own_rows, d = residual_in.shape
    ff = down_weight.shape[0]
    gk = gate_weight.shape[0]
    ff_pad = -(-ff // HD) * HD
    half = HD // 2
    half_n = n // 2
    inverse = 10000.0 ** (-np.arange(0, half, 2, dtype=np.float32) / half)
    inverse = jnp.asarray(np.tile(np.repeat(inverse, 2), 2)[None].astype(np.float32))
    vmem = pl.BlockSpec(memory_space=pltpu.VMEM)
    dma = pltpu.SemaphoreType.DMA
    scratch = [
        pltpu.VMEM((n, tok, 2 * HD), BF16),
        pltpu.VMEM((tok, HD), BF16),
        pltpu.VMEM((tok, HD), F32),
        pltpu.VMEM((tok, HD), F32),
        pltpu.VMEM((tok, HD), F32),
        pltpu.VMEM((ROWS_ATT, tok), F32),
        pltpu.VMEM((ROWS_ATT, tok), F32),
        pltpu.VMEM((ROWS_ATT, HD), F32),
        pltpu.VMEM((ROWS_ATT, HD), F32),
        pltpu.VMEM((tok // GRID_W, HD), F32),
        pltpu.VMEM((tok // GRID_W, HD), F32),
        pltpu.VMEM((2 * ff_pad, n * gk), BF16),
        pltpu.VMEM((ff, n * HD), BF16),
        pltpu.VMEM(out_weight.shape, BF16),
        pltpu.VMEM((tok, d), BF16),
        pltpu.VMEM((tok, HQ * HD), BF16),
        pltpu.VMEM((tok, d), BF16),
        pltpu.VMEM((own_rows, d), F32),
        pltpu.VMEM((4, ROWS_FF, ff), BF16),
        pltpu.VMEM((ROWS_FF, d), F32),
        pltpu.VMEM((4, own_rows, d), BF16),
        pltpu.VMEM((4, own_rows, d), BF16),
        pltpu.VMEM((4, own_rows, d), F32),
        pltpu.VMEM((6, own_rows, d // 2), BF16),
        pltpu.VMEM((6, own_rows, d // 2), BF16),
        dma,
        dma((half_n + 1,)),
        dma((half_n + 1, 2, 2)),
        dma((half_n + 1, 2)),
        dma((half_n + 1, 2)),
        dma((2, half_n + 1)),
        dma((2, half_n + 1)),
        dma,
        dma,
        dma((12,)),
        dma,
        dma((11,)),
        dma,
        dma((10,)),
    ]
    specs = [vmem] * 12
    specs[6] = pl.BlockSpec(memory_space=pl.ANY)
    return pl.pallas_call(
        functools.partial(layer_kernel, n, n_tp),
        out_shape=jax.ShapeDtypeStruct((own_rows, d), BF16),
        in_specs=specs,
        out_specs=vmem,
        scratch_shapes=scratch,
        compiler_params=pltpu.CompilerParams(
            collective_id=0, has_side_effects=True, vmem_limit_bytes=67043328
        ),
        name="layer",
    )(
        queries,
        keys,
        values,
        query_gain[None],
        key_gain[None],
        inverse,
        out_weight,
        residual_in,
        norm_gain[None],
        gate_weight.T,
        up_weight.T,
        down_weight,
    )


def solution(mesh):
    placed = (
        P(("grp", "sp"), "tp"),
        P(("grp", "sp"), None),
        P(("grp", "sp"), None),
        P(),
        P(),
        P(),
        P(("grp", "sp", "tp"), None),
        P(),
        P("sp", "tp"),
        P("sp", "tp"),
        P("tp", "sp"),
    )
    return jax.shard_map(
        functools.partial(local, mesh.shape["sp"], mesh.shape["tp"]),
        mesh=mesh,
        in_specs=placed,
        out_specs=P(("grp", "sp", "tp"), None),
        check_vma=False,
    )
```

```python
import functools
import math

import jax
import jax.numpy as jnp
import numpy as np
from jax import lax
from jax.experimental import pallas as pl
from jax.experimental.pallas import tpu as pltpu
from jax.sharding import PartitionSpec as P

HQ = 8
KV = 2
HD = 128
GRID_W = 64
MESH = pl.DeviceIdType.MESH
F32 = jnp.float32
BF16 = jnp.bfloat16
ROWS_ATT = 256
ROWS_FF = 256
TILES = 4


def scoped(name):
    def wrapped(f):
        def call(*args):
            with jax.named_scope(name):
                return f(*args)

        return call

    return wrapped


def layer_kernel(
    n,
    n_tp,
    q_ref,
    k_ref,
    v_ref,
    qg_ref,
    kg_ref,
    inv_ref,
    ow_hbm,
    res_ref,
    ng_ref,
    gate_ref,
    up_ref,
    down_ref,
    out_ref,
    kv,
    qrot,
    acc,
    mx,
    ls,
    sa,
    sb,
    ta,
    tb,
    cosr,
    sinr,
    gu,
    dw,
    ow,
    res,
    att,
    nrm,
    mid,
    hid,
    part,
    d2s,
    d2r,
    yk,
    xs,
    xr,
    ow_sem,
    kv_ss,
    kv_rs,
    kx_rs,
    kd_rs,
    w_ss,
    w_rs,
    y_rs,
    a_ss,
    a_rs,
    r_ss,
    r_rs,
    t_ss,
    t_rs,
):
    me = lax.axis_index("sp")
    tp = lax.axis_index("tp")
    grp = lax.axis_index("grp")
    odd = lax.rem(grp, 2)
    core = lax.rem(tp, 2)
    x = tp // 2
    tok = q_ref.shape[0]
    d = res_ref.shape[1]
    own_rows = res_ref.shape[0]
    half_n = n // 2
    kv_head = tp // (n_tp // KV)

    def wrap(i):
        return lax.rem(i + n, n)

    right = wrap(me + 1)
    left = wrap(me - 1)
    n1x = x + 1 - 2 * lax.rem(x, 2)
    n2x = 3 - x
    dgx = 3 - n1x
    mate = x * 2 + 1 - core
    n1 = n1x * 2 + core
    n2 = n2x * 2 + core
    dg = dgx * 2 + core
    to_right, to_left = {"sp": right}, {"sp": left}
    to_mate, to_n1, to_n2 = {"tp": mate}, {"tp": n1}, {"tp": n2}
    to_twin = {"grp": grp + 1 - 2 * odd}

    def remote(src, dst, ss, rs, dev):
        return pltpu.make_async_remote_copy(
            src_ref=src, dst_ref=dst, send_sem=ss, recv_sem=rs, device_id=dev, device_id_type=MESH
        )

    def arrived(span, sem):
        pltpu.make_async_copy(span, span, sem).wait()

    load_ow = pltpu.make_async_copy(ow_hbm, ow, ow_sem)
    load_ow.start()

    barrier = pltpu.get_barrier_semaphore()
    for dev in (to_right, to_left, to_mate, to_n1, to_n2, to_twin):
        pl.semaphore_signal(barrier, inc=1, device_id=dev, device_id_type=MESH)

    grid_rows = tok // GRID_W
    lane = lax.broadcasted_iota(jnp.int32, (GRID_W, HD), 1)
    row_pos = (me * grid_rows + lax.broadcasted_iota(jnp.int32, (grid_rows, HD), 0)).astype(F32)
    row_ang = row_pos * inv_ref[...]
    cosr[...] = jnp.cos(row_ang)
    sinr[...] = jnp.sin(row_ang)
    col_ang = lax.broadcasted_iota(jnp.int32, (GRID_W, HD), 0).astype(F32) * inv_ref[...]
    cos_col = jnp.cos(col_ang)
    sin_col = jnp.sin(col_ang)
    even = lax.rem(lane, 2) == 0
    by_row = lane < HD // 2

    def turned(source, gain, i):
        v = source.astype(F32)
        v = v * lax.rsqrt(jnp.mean(v * v, axis=-1, keepdims=True) + 1e-06) * gain
        cosine = jnp.where(by_row, cosr[pl.ds(i, 1), :], cos_col)
        sine = jnp.where(by_row, sinr[pl.ds(i, 1), :], sin_col)
        swapped = jnp.where(even, pltpu.roll(v, HD - 1, 1), pltpu.roll(v, 1, 1))
        signed = jnp.where(even, -sine, sine)
        return (v * cosine + swapped * signed).astype(BF16)

    kv_lanes = pl.ds(pl.multiple_of(kv_head * HD, HD), HD)

    def prep_k(o, _):
        for u in range(TILES):
            i = o * TILES + u
            rows = pl.ds(pl.multiple_of(i * GRID_W, GRID_W), GRID_W)
            kv[me, rows, 0:HD] = turned(k_ref[rows, kv_lanes], kg_ref[...], i)
            kv[me, rows, HD : 2 * HD] = v_ref[rows, kv_lanes]
        return 0

    with jax.named_scope("prepk"):
        lax.fori_loop(0, grid_rows // TILES, prep_k, 0)
        res[pl.ds(pl.multiple_of(tp * own_rows, own_rows), own_rows), :] = res_ref[...]
    with jax.named_scope("barrier"):
        pl.semaphore_wait(barrier, 6)

    quarter = tok // 4
    slab = tok // 2

    side = lax.rem(x, 2)
    share = quarter * 5 // 16
    sizes = (share, share, quarter - 2 * share)

    def block_at(direction, t):
        return wrap(me - t) if direction == 0 else wrap(me + t)

    def piece(direction, t, a, c, which):
        start = (side * share, (1 - side) * share, 2 * share)[which]
        at = pl.multiple_of((2 * a + c) * quarter + start, 16)
        return kv.at[block_at(direction, t), pl.ds(at, sizes[which]), :]

    def kv_ring(direction, t, a, which, late):
        s = piece(direction, t, a, core, which)
        return remote(
            s,
            s,
            kv_ss.at[t],
            kv_rs.at[t + late, a, which // 2],
            (to_right, to_left)[direction],
        )

    def kv_near(direction, t, a, which):
        s = piece(direction, t, a, core, which)
        return remote(s, s, kv_ss.at[t], kx_rs.at[t, a], to_n1)

    def kv_mate(direction, t, a, c, which):
        s = piece(direction, t, a, c, which)
        return remote(s, s, kv_ss.at[t], kd_rs.at[t, a], to_mate)

    def kv_span(rows):
        return kv.at[0, 0:rows]

    for a in range(2):
        for which in (0, 2):
            for direction in range(2):
                kv_ring(direction, 0, a, which, 1).start()

    strips = 8
    strip = d // strips

    def res_slot(j, h=None):
        rows = pl.ds(pl.multiple_of(j * own_rows, own_rows), own_rows)
        if h is None:
            return res.at[rows, :]
        return res.at[rows, pl.ds(pl.multiple_of(h * strip, strip), strip)]

    def pair(s, ss, rs, i, dev):
        return remote(s, s, ss, rs.at[i], dev)

    def other(j):
        return j + 1 - 2 * core

    def res_to_n1(j, h):
        return pair(res_slot(j, h), r_ss, r_rs, h, to_n1)

    def res_on(j, h):
        return pair(res_slot(j, h), r_ss, r_rs, strips, to_n2)

    def res_to_n2(j):
        return pair(res_slot(j), r_ss, r_rs, strips + 1, to_n2)

    def res_mate(j, i):
        return pair(res_slot(j), r_ss, r_rs, strips + 2, to_mate)

    def att_slot(j, i):
        lanes = pl.ds(pl.multiple_of(j * HD, HD), HD)
        return att.at[i * ROWS_ATT : (i + 1) * ROWS_ATT, lanes]

    def att_to(j, i, which):
        return pair(att_slot(j, i), a_ss, a_rs, i, (to_n1, to_n2)[which])

    def att_on(j, i):
        return pair(att_slot(j, i), a_ss, a_rs, 4 + i, to_n2 if i < 2 else to_n1)

    def att_mate(j, i, which):
        return pair(att_slot(j, i), a_ss, a_rs, 8 + i, to_mate)

    def att_send(i):
        att_to(tp, i, 0).start()
        att_to(tp, i, 1).start()
        att_mate(tp, i, 0).start()

    def att_relay(i):
        arrived(att.at[0:ROWS_ATT, 0 : 2 * HD], a_rs.at[i])
        att_on(n1 if i < 2 else n2, i).start()
        att_mate(n1, i, 1).start()
        att_mate(n2, i, 2).start()

    def att_diag(i):
        att_on(dg, i).wait_recv()
        att_mate(dg, i, 3).start()

    def att_taken(i):
        arrived(att.at[0:ROWS_ATT, 0 : 4 * HD], a_rs.at[8 + i])

    def res_pass(h):
        res_to_n1(n1, h).wait_recv()
        res_on(n1, h).start()

    res_to_n2(tp).start()
    res_mate(tp, 0).start()

    gk = gate_ref.shape[1]
    ff = down_ref.shape[0]
    ff_pad = gu.shape[0] // 2

    def w_slot(which, b):
        if which == 2:
            return dw.at[:, pl.ds(pl.multiple_of(b * HD, HD), HD)]
        lanes = pl.ds(pl.multiple_of(b * gk, gk), gk)
        row = (odd if which == 0 else 1 - odd) * ff_pad
        return gu.at[pl.ds(pl.multiple_of(row, ff_pad), ff), lanes]

    def w_copy(which, direction, t, late):
        s = w_slot(which, block_at(direction, t))
        return remote(
            s,
            s,
            w_ss.at[which // 2, t],
            w_rs.at[which // 2, t + late],
            (to_right, to_left)[direction],
        )

    def w_twin(which, direction, t):
        s = w_slot(which, block_at(direction, t))
        return remote(s, s, w_ss.at[0, t], y_rs, to_twin)

    def w_span(which, count):
        return (gu, None, dw)[which].at[0:ff, 0 : count * gk]

    def w_start(whiches):
        for which in whiches:
            for direction in range(2):
                w_copy(which, direction, 0, 1).start()

    @scoped("wstep")
    def w_step(whiches, t):
        for which in whiches:
            arrived(w_span(which, 2), w_rs.at[which // 2, t])
            for direction in range(2):

                @pl.when((t < half_n - 1) | (core == direction))
                def _():
                    w_copy(which, direction, t, 1).start()

                if which == 0:
                    w_twin(0, direction, t).start()

    def w_last(which):
        for direction in range(2):

            @pl.when(core == direction)
            def _():
                arrived(w_span(which, 1), w_rs.at[which // 2, half_n])
                if which == 0:
                    w_twin(0, direction, half_n).start()

    w_order = [(2, 2)]
    for t in range(4, half_n + 1):
        w_order += [(0, t), (2, t - 1)]
    w_order += [(2, half_n)]

    @scoped("pump")
    def pump(count=1):
        for _ in range(count):
            which, t = w_order.pop(0)
            if t < half_n:
                w_step((which,), t)
            else:
                w_last(which)

    @scoped("wtwin")
    def w_taken():
        arrived(w_span(0, n - 1), y_rs)

    def w_sent():
        for t in range(half_n + 1):
            ring = 2 if t < half_n - 1 else half_n - t
            twin = 0 if t == 0 else 2 if t < half_n else 1
            arrived(w_span(0, ring + twin), w_ss.at[0, t])
            if ring > 0:
                arrived(w_span(2, ring), w_ss.at[1, t])

    def prep_q(o, _):
        for u in range(TILES):
            i = o * TILES + u
            rows = pl.ds(pl.multiple_of(i * GRID_W, GRID_W), GRID_W)
            qrot[rows, :] = turned(q_ref[rows, :], qg_ref[...], i)
        return 0

    with jax.named_scope("prepq"):
        lax.fori_loop(0, grid_rows // TILES, prep_q, 0)
    own_lanes = pl.ds(pl.multiple_of(me * gk, gk), gk)
    gu[0:ff, own_lanes] = gate_ref[...]
    gu[ff_pad : ff_pad + ff, own_lanes] = up_ref[...]
    dw[:, pl.ds(pl.multiple_of(me * HD, HD), HD)] = down_ref[...]
    for which in range(2):
        gu[which * ff_pad + ff : (which + 1) * ff_pad, :] = jnp.zeros((ff_pad - ff, gu.shape[1]), BF16)
    mx[...] = jnp.full(mx.shape, -1e30, F32)
    ls[...] = jnp.zeros(ls.shape, F32)
    acc[...] = jnp.zeros(acc.shape, F32)

    factor = HD ** (-0.5) * math.log2(math.e)

    dims = (((1,), (1,)), ((), ()))
    blocks = tok // ROWS_ATT

    def slabs(keys):
        return [(b, pl.ds(pl.multiple_of(h * slab, slab), slab)) for b, h in keys]

    def score(keys, i, s_ref, t_ref):
        q = qrot[i * ROWS_ATT : (i + 1) * ROWS_ATT, :]
        top = None
        for n_slab, (b, r) in enumerate(slabs(keys)):
            s = lax.dot_general(q, kv[b, r, 0:HD], dims, preferred_element_type=F32)
            s_ref[:, n_slab * slab : (n_slab + 1) * slab] = s
            for j in range(slab // HD):
                tile = s[:, j * HD : (j + 1) * HD]
                top = tile if top is None else jnp.maximum(top, tile)
        t_ref[...] = top

    def weigh(keys, i, s_ref, t_ref):
        rows = slice(i * ROWS_ATT, (i + 1) * ROWS_ATT)
        old = mx[rows, :]
        new = jnp.maximum(old, jnp.max(t_ref[...], axis=1, keepdims=True))
        mx[rows, :] = new
        alpha = jnp.exp2((old - new) * factor)
        base = new[:, 0:1]
        total = ls[rows, :] * alpha
        weighted = acc[rows, :] * alpha
        for n_slab, (b, r) in enumerate(slabs(keys)):
            raised = jnp.exp2((s_ref[:, n_slab * slab : (n_slab + 1) * slab] - base) * factor)
            for j in range(slab // HD):
                total = total + raised[:, j * HD : (j + 1) * HD]
            weighted = weighted + jnp.dot(
                raised.astype(BF16), kv[b, r, HD : 2 * HD], preferred_element_type=F32
            )
        ls[rows, :] = total
        acc[rows, :] = weighted

    held = ((sa, ta), (sb, tb))

    def attend_units(units, after=None):
        score(*units[0], *held[0])
        for u, unit in enumerate(units):
            if u + 1 < len(units):
                score(*units[u + 1], *held[(u + 1) % 2])
            weigh(*unit, *held[u % 2])
            if after is not None:
                after(u)

    def keys_of(t, a):
        return ((wrap(me - t), a), (wrap(me + t), a))

    @scoped("attend")
    def attend(keys):
        attend_units([(keys, i) for i in range(blocks)])

    @scoped("take")
    def kv_take(t, a):
        for which in (0, 2):
            arrived(kv_span(2 * sizes[which]), kv_rs.at[t, a, which // 2])
            for direction in range(2):

                @pl.when((t < half_n - 1) | (core == direction))
                def _():
                    kv_ring(direction, t, a, which, 1).start()

                if which == 0:
                    kv_near(direction, t, a, 0).start()
                kv_mate(direction, t, a, core, which).start()

    @scoped("near")
    def near_take(t, a):
        arrived(kv_span(2 * share), kx_rs.at[t, a])
        for direction in range(2):
            kv_mate(direction, t, a, core, 1).start()

    @scoped("mate")
    def mate_take(t, a):
        arrived(kv_span(2 * quarter), kd_rs.at[t, a])

    def on_last(who, f):
        for direction in range(2):

            @pl.when(who == direction)
            def _():
                for a in range(2):
                    f(direction, a)

    attend(((me, 0), (me, 1)))
    kv_take(1, 0)
    kv_take(1, 1)
    kv_take(2, 0)
    near_take(1, 0)

    def phase(p, _):
        kv_take((p + 1) // 2, lax.rem(p + 1, 2))

        @pl.when(p < 8)
        def _():
            res_to_n1(tp, p - 4).start()

        @pl.when((lax.rem(p, 2) == 0) & (p >= 8))
        def _():
            res_to_n1(tp, p // 2).start()

        @pl.when(p >= 8)
        def _():
            res_pass(p - 8)

        @pl.when(p == 8)
        def _():
            w_start((0,))

        @pl.when((lax.rem(p, 2) == 0) & (p >= 10))
        def _():
            w_step((0,), (p - 8) // 2)

        @pl.when(p == 9)
        def _():
            w_start((2,))

        @pl.when(p == 13)
        def _():
            w_step((2,), 1)

        @pl.when(p == half_n)
        def _():
            res_to_n2(n2).wait_recv()
            res_mate(n2, 1).start()

        near_take((p - 1) // 2, lax.rem(p - 1, 2))
        tb, ab = (p - 2) // 2, lax.rem(p, 2)
        mate_take(tb, ab)
        attend(keys_of(tb, ab))
        return 0

    lax.fori_loop(4, 2 * half_n - 1, phase, 0)

    def last_take(direction, a):
        for which in (0, 2):
            arrived(kv_span(sizes[which]), kv_rs.at[half_n, a, which // 2])
            if which == 0:
                kv_near(direction, half_n, a, 0).start()
            kv_mate(direction, half_n, a, core, which).start()

    def last_near(direction, a):
        arrived(kv_span(share), kx_rs.at[half_n, a])
        kv_mate(direction, half_n, a, core, 1).start()

    def last_mate(direction, a):
        arrived(kv_span(quarter), kd_rs.at[half_n, a])

    with jax.named_scope("lasttake"):
        on_last(core, last_take)
    near_take(half_n - 1, 0)
    mate_take(half_n - 2, 1)
    near_take(half_n - 1, 1)
    mate_take(half_n - 1, 0)
    pump()
    relay, diag, taken = scoped("relay")(att_relay), scoped("diag")(att_diag), scoped("taken")(att_taken)

    last_keys = (
        keys_of(half_n - 2, 1),
        keys_of(half_n - 1, 0),
        keys_of(half_n - 1, 1),
        ((wrap(me + half_n), 0), (wrap(me + half_n), 1)),
    )
    order = [(0, 0), (1, 0), (2, 0), (0, 1), (3, 0), (1, 1), (2, 1), (3, 1)]
    order += [(g, i) for i in range(2, blocks) for g in range(4)]

    def finish(u):
        if u == 0:
            mate_take(half_n - 1, 1)
        if u == 1:
            with jax.named_scope("lastnear"):
                on_last(core, last_near)
            res_pass(7)
            res_mate(n1, 2).start()
        if u == 2:
            with jax.named_scope("lastmate"):
                on_last(1 - core, last_mate)
        if u > 0 and order[u - 1][0] == 3:
            att_send(order[u - 1][1])
        g, i = order[u]
        if g != 3:
            return
        rows = slice(i * ROWS_ATT, (i + 1) * ROWS_ATT)
        below = jnp.sum(ls[rows, :], axis=1, keepdims=True)
        att[rows, pl.ds(pl.multiple_of(tp * HD, HD), HD)] = (acc[rows, :] / below).astype(BF16)
        pump()
        if i == 2:
            relay(0)

    with jax.named_scope("lastattend"):
        attend_units([(last_keys[g], i) for g, i in order], finish)
    att_send(blocks - 1)
    with jax.named_scope("resdiag"):
        arrived(res.at[0:own_rows], r_rs.at[strips])
        res_mate(dg, 3).start()
    load_ow.wait()

    @scoped("project")
    def project(i):
        rows = slice(i * ROWS_FF, (i + 1) * ROWS_FF)
        middle = res[rows, :].astype(F32) + jnp.dot(
            att[rows, :], ow[...], preferred_element_type=F32
        )
        scale = lax.rsqrt(jnp.mean(middle * middle, axis=-1, keepdims=True) + 1e-06)
        nrm[rows, :] = (middle * scale * ng_ref[...]).astype(BF16)
        for j in range(2):

            @pl.when(tp == 2 * i + j)
            def _():
                mid[...] = middle[j * own_rows : (j + 1) * own_rows, :]

    relay(1)
    pump()
    diag(0)
    relay(2)
    pump()
    with jax.named_scope("resmate"):
        arrived(res.at[0 : 4 * own_rows], r_rs.at[strips + 2])
    taken(0)
    project(0)
    relay(3)
    diag(1)
    pump()
    taken(1)
    project(1)
    diag(2)
    pump()
    taken(2)
    project(2)
    diag(3)
    pump()
    taken(3)
    project(3)
    pump()
    w_taken()

    half_d = d // 2
    cols = (slice(0, half_d), slice(half_d, d))
    owners = (dgx, n1x, n2x, x)

    def d2_copy(o):
        return remote(d2s.at[o], d2r.at[o], t_ss, t_rs.at[o], to_mate)

    def x_copy(m):
        dev = (to_n1, to_n2, to_n1, to_n1, to_n2, to_n2)[m]
        return remote(xs.at[m], xr.at[m], t_ss, t_rs.at[4 + m], dev)

    @scoped("units")
    def units(o):
        rows = pl.ds(pl.multiple_of(owners[o] * ROWS_FF, ROWS_FF), ROWS_FF)
        act = lax.dot_general(nrm[rows, :], gu[...], dims, preferred_element_type=F32)
        gate = act[:, 0:ff]
        hid[o] = (gate / (1.0 + jnp.exp(-gate)) * act[:, ff_pad : ff_pad + ff]).astype(BF16)

    @scoped("block")
    def block(o):
        part[...] = jnp.dot(hid[o], dw[...], preferred_element_type=F32)
        theirs = pl.ds(pl.multiple_of((1 - core) * own_rows, own_rows), own_rows)
        mine = pl.ds(pl.multiple_of(core * own_rows, own_rows), own_rows)
        d2s[o] = part[theirs, :].astype(BF16)
        yk[o] = part[mine, :]
        d2_copy(o).start()

    def both(o, c):
        return yk[o, :, cols[c]] + d2r[o, :, cols[c]].astype(F32)

    @scoped("sums")
    def sums(o):
        d2_copy(o).wait_recv()
        if o == 0:
            for c in range(2):
                xs[c] = both(0, c).astype(BF16)
                x_copy(c).start()
        elif o == 1:
            xs[2] = both(1, 0).astype(BF16)
            x_copy(2).start()
            yk[1, :, cols[1]] = both(1, 1)
        elif o == 2:
            xs[4] = both(2, 1).astype(BF16)
            x_copy(4).start()
            yk[2, :, cols[0]] = both(2, 0)
        else:
            for c in range(2):
                yk[3, :, cols[c]] = both(3, c) + mid[:, cols[c]]

    units(0)
    units(1)
    units(2)
    pump()
    units(3)
    pump(len(w_order))
    block(0)
    sums(0)
    block(1)
    block(2)
    sums(1)
    block(3)
    sums(2)
    sums(3)
    with jax.named_scope("pass"):
        x_copy(1).wait_recv()
        xs[3] = (yk[1, :, cols[1]] + xr[1].astype(F32)).astype(BF16)
        x_copy(3).start()
        x_copy(0).wait_recv()
        xs[5] = (yk[2, :, cols[0]] + xr[0].astype(F32)).astype(BF16)
        x_copy(5).start()
    for t in range(half_n + 1):
        ring = (2 if t < half_n - 1 else half_n - t) * 2 * (quarter - share)
        others = 0 if t == 0 else (2 if t < half_n else 1) * 2 * (share + quarter)
        arrived(kv.at[0:2, 0 : (ring + others) // 2], kv_ss.at[t])
    w_sent()
    arrived(res.at[0 : 7 * own_rows], r_ss)
    arrived(att.at[:, 0 : 7 * HD], a_ss)
    with jax.named_scope("final"):
        for c, (m1, m2) in enumerate(((2, 5), (4, 3))):
            x_copy(m1).wait_recv()
            x_copy(m2).wait_recv()
            out_ref[:, cols[c]] = (
                yk[3, :, cols[c]] + xr[m1].astype(F32) + xr[m2].astype(F32)
            ).astype(BF16)

    arrived(res.at[0 : 7 * own_rows], t_ss)


def local(
    n,
    n_tp,
    queries,
    keys,
    values,
    query_gain,
    key_gain,
    out_weight,
    residual_in,
    norm_gain,
    gate_weight,
    up_weight,
    down_weight,
):
    tok = queries.shape[0]
    own_rows, d = residual_in.shape
    ff = down_weight.shape[0]
    gk = gate_weight.shape[0]
    ff_pad = -(-ff // HD) * HD
    half = HD // 2
    half_n = n // 2
    inverse = 10000.0 ** (-np.arange(0, half, 2, dtype=np.float32) / half)
    inverse = jnp.asarray(np.tile(np.repeat(inverse, 2), 2)[None].astype(np.float32))
    vmem = pl.BlockSpec(memory_space=pltpu.VMEM)
    dma = pltpu.SemaphoreType.DMA
    scratch = [
        pltpu.VMEM((n, tok, 2 * HD), BF16),
        pltpu.VMEM((tok, HD), BF16),
        pltpu.VMEM((tok, HD), F32),
        pltpu.VMEM((tok, HD), F32),
        pltpu.VMEM((tok, HD), F32),
        pltpu.VMEM((ROWS_ATT, tok), F32),
        pltpu.VMEM((ROWS_ATT, tok), F32),
        pltpu.VMEM((ROWS_ATT, HD), F32),
        pltpu.VMEM((ROWS_ATT, HD), F32),
        pltpu.VMEM((tok // GRID_W, HD), F32),
        pltpu.VMEM((tok // GRID_W, HD), F32),
        pltpu.VMEM((2 * ff_pad, n * gk), BF16),
        pltpu.VMEM((ff, n * HD), BF16),
        pltpu.VMEM(out_weight.shape, BF16),
        pltpu.VMEM((tok, d), BF16),
        pltpu.VMEM((tok, HQ * HD), BF16),
        pltpu.VMEM((tok, d), BF16),
        pltpu.VMEM((own_rows, d), F32),
        pltpu.VMEM((4, ROWS_FF, ff), BF16),
        pltpu.VMEM((ROWS_FF, d), F32),
        pltpu.VMEM((4, own_rows, d), BF16),
        pltpu.VMEM((4, own_rows, d), BF16),
        pltpu.VMEM((4, own_rows, d), F32),
        pltpu.VMEM((6, own_rows, d // 2), BF16),
        pltpu.VMEM((6, own_rows, d // 2), BF16),
        dma,
        dma((half_n + 1,)),
        dma((half_n + 1, 2, 2)),
        dma((half_n + 1, 2)),
        dma((half_n + 1, 2)),
        dma((2, half_n + 1)),
        dma((2, half_n + 1)),
        dma,
        dma,
        dma((12,)),
        dma,
        dma((11,)),
        dma,
        dma((10,)),
    ]
    specs = [vmem] * 12
    specs[6] = pl.BlockSpec(memory_space=pl.ANY)
    return pl.pallas_call(
        functools.partial(layer_kernel, n, n_tp),
        out_shape=jax.ShapeDtypeStruct((own_rows, d), BF16),
        in_specs=specs,
        out_specs=vmem,
        scratch_shapes=scratch,
        compiler_params=pltpu.CompilerParams(
            collective_id=0, has_side_effects=True, vmem_limit_bytes=67043328
        ),
        name="layer",
    )(
        queries,
        keys,
        values,
        query_gain[None],
        key_gain[None],
        inverse,
        out_weight,
        residual_in,
        norm_gain[None],
        gate_weight.T,
        up_weight.T,
        down_weight,
    )


def solution(mesh):
    placed = (
        P(("grp", "sp"), "tp"),
        P(("grp", "sp"), None),
        P(("grp", "sp"), None),
        P(),
        P(),
        P(),
        P(("grp", "sp", "tp"), None),
        P(),
        P("sp", "tp"),
        P("sp", "tp"),
        P("tp", "sp"),
    )
    return jax.shard_map(
        functools.partial(local, mesh.shape["sp"], mesh.shape["tp"]),
        mesh=mesh,
        in_specs=placed,
        out_specs=P(("grp", "sp", "tp"), None),
        check_vma=False,
    )
```
